32 devices in a mesh: sp: 8 (over z, y), tp: 4 (over x, core).
Axes of the slice: x: 2, y: 2, z: 4, core: 2. Of those that a mesh axis runs over, the one named last changes fastest.
Arguments:
- skip_trunk_vector: bfloat16 [4096, 2048], P('sp', 'tp'), may hold values from -16 to 16
- valve_preactivation: bfloat16 [4096, 2048], P('sp', 'tp'), may hold values from -6 to 6
- projected_heads_payload: bfloat16 [4096, 2048], P('sp', 'tp'), may hold values from -6 to 6
- cluster_ingests: bfloat16 [4096, 1024], P('sp', 'tp'), may hold values from -6 to 6
- cluster_observers: bfloat16 [4096, 1024], P('sp', 'tp'), may hold values from -6 to 6
- pre_softplus_increments: float32 [2, 4096, 32], P(None, 'sp', 'tp'), may hold values from -6 to 6
- attenuation_ln_rate: float32 [2, 32], P(None, 'tp'), may hold values from -13 to -3
- additional_attenuation: float32 [2, 4096, 32], P(None, 'sp', 'tp'), may hold values from -3 to 0
- payload_conv_weights: float32 [7, 2048], P(None, 'tp'), may hold values from -2 to 2
- ingest_conv_weights: float32 [7, 1024], P(None, 'tp'), may hold values from -2 to 2
- observer_conv_weights: float32 [7, 1024], P(None, 'tp'), may hold values from -2 to 2
- valved_cluster_factor: float32 [2048], P('tp'), may hold values from 0.1 to 1.9
- closing_map_matrix: bfloat16 [2048, 2048], P('tp'), may hold values from -0.125 to 0.125
- dense_standardize_factor: float32 [2048], replicated, may hold values from 0.1 to 1.9
- dense_valve_map: bfloat16 [2048, 5120], P('sp', 'tp'), may hold values from -0.125 to 0.125
- dense_payload_map: bfloat16 [2048, 5120], P('sp', 'tp'), may hold values from -0.125 to 0.125
- valve_series_smoother: float32 [3, 5120], P(None, 'tp'), may hold values from -3.5 to 3.5
- payload_series_smoother: float32 [3, 5120], P(None, 'tp'), may hold values from -3.5 to 3.5
- dense_contract_map: bfloat16 [5120, 2048], P('tp', 'sp'), may hold values from -0.078125 to 0.078125
Outputs:
- updated: bfloat16 [4096, 2048], P('sp', 'tp')
The draws below stay inside these ranges and needn't reach their ends.
All inputs are finite; a program needn't handle non-finite values.
Results may differ from the reference program's by a relative error of at most 0.019.
Values may be sent and summed in bfloat16 or wider, within the bound.
No kernel may reach another device: no remote copies, remote signals or barrier semaphores. Data moves between devices by JAX's collectives and lax.ppermute only.
A program may use at most 64 MiB of HBM per device.

```python
import jax
import jax.numpy as jnp
from jax import lax

TOK_DEV = 512
D = 2048
HEADS = 32
HEAD_DIM = 64
GROUPS = 8
STATE = 128
CONV = 7
FF = 5120
FF_TAPS = 3
MIXING_WIDTH = 2048
SEQUENCE_SPAN = 4096
N_TP = 4


def draw_skip_trunk_vector(key, part):
    column = jnp.arange(D, dtype=jnp.float32) / D
    scales = 0.5 * jnp.exp(jnp.log(5.0) * column)
    random_part = jax.random.truncated_normal(key, -6.0, 6.0, (SEQUENCE_SPAN, D), jnp.float32)
    return (random_part * scales).astype(jnp.bfloat16)


def draw_pre_softplus_increments(key, part):
    key_one, key_two = jax.random.split(key)
    blocks = SEQUENCE_SPAN // TOK_DEV
    offsets = jax.random.uniform(key_two, (2, blocks, 1, HEADS), jnp.float32, -1.2, 1.2)
    spread = jnp.broadcast_to(offsets, (2, blocks, TOK_DEV, HEADS)).reshape(2, SEQUENCE_SPAN, HEADS)
    random_part = jax.random.truncated_normal(key_one, -4.0, 4.0, (2, SEQUENCE_SPAN, HEADS), jnp.float32)
    return random_part + spread


def draw_attenuation_ln_rate(key, part):
    key_one, key_two, key_three = jax.random.split(key, 3)
    quick = jax.random.bernoulli(key_one, 0.5, (2, HEADS))
    slow_rate = jax.random.uniform(key_two, (2, HEADS), jnp.float32, 0.5, 1.0) * (0.6 / SEQUENCE_SPAN)
    fast_rate = jnp.exp(jax.random.uniform(key_three, (2, HEADS), jnp.float32, jnp.log(1.0 / 60.0), jnp.log(1.0 / 25.0)))
    return jnp.log(jnp.where(quick, fast_rate, slow_rate))


def draw_additional_attenuation(key, part):
    key_one, key_two = jax.random.split(key)
    places = jax.random.randint(key_one, (2, 4), 0, SEQUENCE_SPAN)
    kept_share = jax.random.uniform(key_two, (2, 4, HEADS), jnp.float32, 0.5, 0.8)
    position = jnp.arange(SEQUENCE_SPAN, dtype=jnp.int32)
    matches = (position[None, :, None] == places[:, None, :]).astype(jnp.float32)
    return jnp.einsum('dtk,dkh->dth', matches, jnp.log(kept_share))


def level_of(stream_key, extent, cuts, low, top_value):
    def one(axis_at, parts):
        heights = jax.random.uniform(jax.random.fold_in(jax.random.fold_in(stream_key, 6), axis_at), (parts,), jnp.float32, low / len(cuts), top_value / len(cuts))
        return jnp.repeat(jnp.exp(heights), extent[axis_at] // parts).reshape((-1,) + (1,) * (len(extent) - axis_at - 1))

    level = one(*cuts[0])
    for cut in cuts[1:]:
        level = level * one(*cut)
    return level


def noise(stream_key, extent, width, limit, cuts=(), held_as=jnp.bfloat16):
    factor_of = level_of(stream_key, extent, cuts, -0.22, 0.18) if cuts else 1.0
    array = jax.random.normal(stream_key, extent, jnp.float32) * width * factor_of
    return jnp.minimum(jnp.maximum(array, -limit), limit).astype(held_as)


def setup_inputs(seed: int = 0) -> dict:
    splits = jax.random.split(jax.random.key(seed), 20)
    return {
        "skip_trunk_vector": draw_skip_trunk_vector(jax.random.fold_in(splits[19], 71), 0),
        "valve_preactivation": noise(splits[1], (SEQUENCE_SPAN, MIXING_WIDTH), 1.0, 6.0, ((0, 8), (1, 4))),
        "projected_heads_payload": noise(splits[2], (SEQUENCE_SPAN, MIXING_WIDTH), 1.0, 6.0, ((0, 8), (1, 4))),
        "cluster_ingests": noise(splits[3], (SEQUENCE_SPAN, GROUPS * STATE), 1.0, 6.0, ((0, 8), (1, 4))),
        "cluster_observers": noise(splits[4], (SEQUENCE_SPAN, GROUPS * STATE), 1.0, 6.0, ((0, 8), (1, 4))),
        "pre_softplus_increments": draw_pre_softplus_increments(jax.random.fold_in(splits[19], 71), 0),
        "attenuation_ln_rate": draw_attenuation_ln_rate(jax.random.fold_in(splits[19], 71), 0),
        "additional_attenuation": draw_additional_attenuation(jax.random.fold_in(splits[19], 71), 0),
        "payload_conv_weights": noise(splits[8], (CONV, MIXING_WIDTH), CONV ** -0.5, 2.0, ((1, 4),), jnp.float32),
        "ingest_conv_weights": noise(splits[9], (CONV, GROUPS * STATE), CONV ** -0.5, 2.0, ((1, 4),), jnp.float32),
        "observer_conv_weights": noise(splits[10], (CONV, GROUPS * STATE), CONV ** -0.5, 2.0, ((1, 4),), jnp.float32),
        "valved_cluster_factor": jnp.clip(1.0 + 0.18 * jax.random.normal(splits[11], (MIXING_WIDTH,), jnp.float32), 0.1, 1.9),
        "closing_map_matrix": noise(splits[12], (MIXING_WIDTH, D), MIXING_WIDTH ** -0.5, 0.125, ((0, 4),)),
        "dense_standardize_factor": jnp.clip(1.0 + 0.18 * jax.random.normal(splits[13], (D,), jnp.float32), 0.1, 1.9),
        "dense_valve_map": noise(splits[14], (D, FF), D ** -0.5, 0.125, ((0, 8), (1, 4))),
        "dense_payload_map": noise(splits[15], (D, FF), D ** -0.5, 0.125, ((0, 8), (1, 4))),
        "valve_series_smoother": noise(splits[16], (FF_TAPS, FF), FF_TAPS ** -0.5, 3.5, ((1, 4),), jnp.float32),
        "payload_series_smoother": noise(splits[17], (FF_TAPS, FF), FF_TAPS ** -0.5, 3.5, ((1, 4),), jnp.float32),
        "dense_contract_map": noise(splits[18], (FF, D), FF ** -0.5, 0.078125, ((0, 4), (1, 8))),
    }


EPSILON = 1e-06

def centred_conv(data, kernel):
    margin = kernel.shape[0] // 2
    length = data.shape[0]
    padded = jnp.pad(data, ((margin, margin), (0, 0)))
    summed = padded[0:length] * kernel[0]
    for offset in range(1, kernel.shape[0]):
        summed = summed + padded[offset:offset + length] * kernel[offset]
    return summed

def one_way(values_f, inputs_h, readout_h, stride_lengths_change, fading_exponent):
    blocks = SEQUENCE_SPAN // TOK_DEV
    places = jnp.arange(TOK_DEV, dtype=jnp.int32)
    lower_mask = places[:, None] >= places[None, :]

    def advance(carried, pieces):
        block_values, block_inputs, block_readout, block_steps, block_logs = pieces
        running = jnp.cumsum(block_logs, axis=0)
        log_gaps = running.T[:, :, None] - running.T[:, None, :]
        decays = jnp.exp(jnp.where(lower_mask[None], log_gaps, -jnp.inf))
        scores = jnp.einsum('thn,shn->hts', block_readout, block_inputs, precision=lax.Precision.HIGHEST)
        weights = scores * decays * block_steps.T[:, None, :]
        within = jnp.einsum('hts,shp->thp', weights, block_values, precision=lax.Precision.HIGHEST)
        outer = jnp.einsum('thn,hpn->thp', block_readout, carried, precision=lax.Precision.HIGHEST)
        outer = outer * jnp.exp(running)[:, :, None]
        to_end = jnp.exp(running[-1][None, :] - running) * block_steps
        block_state = jnp.einsum('sh,shp,shn->hpn', to_end, block_values, block_inputs, precision=lax.Precision.HIGHEST)
        carried = carried * jnp.exp(running[-1])[:, None, None] + block_state
        return (carried, within + outer)
    pieces = (values_f.reshape(blocks, TOK_DEV, HEADS, HEAD_DIM), inputs_h.reshape(blocks, TOK_DEV, HEADS, STATE), readout_h.reshape(blocks, TOK_DEV, HEADS, STATE), stride_lengths_change.reshape(blocks, TOK_DEV, HEADS), fading_exponent.reshape(blocks, TOK_DEV, HEADS))
    start_state = jnp.zeros((HEADS, HEAD_DIM, STATE), jnp.float32)
    final_state, results = lax.scan(advance, start_state, pieces)
    return results.reshape(SEQUENCE_SPAN, HEADS, HEAD_DIM)

def split_product(left, right, part_width, out_width):

    def add_part(summed, index):
        start = index * part_width
        columns = lax.dynamic_slice_in_dim(left, start, part_width, 1)
        rows_part = lax.dynamic_slice_in_dim(right, start, part_width, 0)
        term = jnp.dot(columns, rows_part, preferred_element_type=jnp.float32).astype(jnp.bfloat16)
        return (summed + lax.optimization_barrier(term).astype(jnp.float32), index)
    zero_sum = jnp.zeros((left.shape[0], out_width), jnp.float32)
    summed, indices = lax.scan(add_part, zero_sum, jnp.arange(N_TP, dtype=jnp.int32))
    return summed

def reference(skip_trunk_vector, valve_preactivation, projected_heads_payload, cluster_ingests, cluster_observers, pre_softplus_increments, attenuation_ln_rate, additional_attenuation, payload_conv_weights, ingest_conv_weights, observer_conv_weights, valved_cluster_factor, closing_map_matrix, dense_standardize_factor, dense_valve_map, dense_payload_map, valve_series_smoother, payload_series_smoother, dense_contract_map):
    per_group = HEADS // GROUPS
    mixed_values = jax.nn.silu(centred_conv(projected_heads_payload.astype(jnp.float32), payload_conv_weights)).astype(jnp.bfloat16)
    mixed_inputs = jax.nn.silu(centred_conv(cluster_ingests.astype(jnp.float32), ingest_conv_weights)).astype(jnp.bfloat16)
    mixed_readout = jax.nn.silu(centred_conv(cluster_observers.astype(jnp.float32), observer_conv_weights)).astype(jnp.bfloat16)
    values_f = mixed_values.astype(jnp.float32).reshape(SEQUENCE_SPAN, HEADS, HEAD_DIM)
    inputs_h = jnp.repeat(mixed_inputs.astype(jnp.float32).reshape(SEQUENCE_SPAN, GROUPS, STATE), per_group, axis=1)
    readout_h = jnp.repeat(mixed_readout.astype(jnp.float32).reshape(SEQUENCE_SPAN, GROUPS, STATE), per_group, axis=1)
    stride_lengths_change = jax.nn.softplus(pre_softplus_increments)
    fading_exponent = additional_attenuation - stride_lengths_change * jnp.exp(attenuation_ln_rate)[:, None, :]
    forward = one_way(values_f, inputs_h, readout_h, stride_lengths_change[0], fading_exponent[0])
    backward = jnp.flip(one_way(jnp.flip(values_f, 0), jnp.flip(inputs_h, 0), jnp.flip(readout_h, 0), jnp.flip(stride_lengths_change[1], 0), jnp.flip(fading_exponent[1], 0)), 0)
    gated = (forward + backward).reshape(SEQUENCE_SPAN, MIXING_WIDTH) * jax.nn.silu(valve_preactivation.astype(jnp.float32))
    grouped = gated.reshape(SEQUENCE_SPAN, GROUPS, MIXING_WIDTH // GROUPS)
    standardized = grouped * lax.rsqrt(lax.optimization_barrier(jnp.mean(grouped * grouped, axis=2, keepdims=True)) + EPSILON)
    blending_result = (standardized.reshape(SEQUENCE_SPAN, MIXING_WIDTH) * valved_cluster_factor).astype(jnp.bfloat16)
    mapped_vector = split_product(blending_result, closing_map_matrix, MIXING_WIDTH // N_TP, D)
    intermediate_hidden = (skip_trunk_vector.astype(jnp.float32) + mapped_vector).astype(jnp.bfloat16)
    middle_f = intermediate_hidden.astype(jnp.float32)
    scaled = middle_f * lax.rsqrt(lax.optimization_barrier(jnp.mean(middle_f * middle_f, axis=1, keepdims=True)) + EPSILON)
    normed_rows = (scaled * dense_standardize_factor).astype(jnp.bfloat16)
    gate_rows = jnp.dot(normed_rows, dense_valve_map, preferred_element_type=jnp.float32).astype(jnp.bfloat16)
    value_rows = jnp.dot(normed_rows, dense_payload_map, preferred_element_type=jnp.float32).astype(jnp.bfloat16)
    gate_conv = centred_conv(gate_rows.astype(jnp.float32), valve_series_smoother)
    value_conv = centred_conv(value_rows.astype(jnp.float32), payload_series_smoother)
    hidden = (jax.nn.silu(gate_conv) * value_conv).astype(jnp.bfloat16)
    down_sum = split_product(hidden, dense_contract_map, FF // N_TP, D)
    return (middle_f + down_sum).astype(jnp.bfloat16)
```

```python
import jax
import jax.numpy as jnp
import numpy as np
from jax import lax
from jax.experimental import pallas as pl
from jax.experimental.pallas import tpu as pltpu
from jax.sharding import PartitionSpec as P

HEADS = 32
GROUPS = 8
STATE = 128
EPSILON = 1e-06
TAIL = 16


def ring_cycle(mesh):
    line = mesh.devices[:, 0].ravel()
    count = len(line)
    if not all(hasattr(d, "coords") for d in line):
        return list(range(count))
    spots = {(d.coords[2], d.coords[1]): i for i, d in enumerate(line)}
    deep = sorted({z for z, _ in spots})
    wide = sorted({y for _, y in spots})
    if len(spots) != count or len(deep) % 2 or len(wide) < 2:
        return list(range(count))
    path = []
    for at, z in enumerate(deep):
        row = wide[1:] if at % 2 == 0 else wide[:0:-1]
        path += [(z, y) for y in row]
    path += [(z, wide[0]) for z in reversed(deep)]
    return [spots[spot] for spot in path]


def bit_reverse(value, bits):
    return int(format(value, f"0{bits}b")[::-1], 2) if bits else 0


class Butterfly:
    def __init__(self, count):
        self.count = count
        self.bits = count.bit_length() - 1
        self.scatter_mask = [bit_reverse(count - 1 - p, self.bits) for p in range(count)]
        self.gather_mask = [bit_reverse(p, self.bits) for p in range(count)]

    def swap(self, array, bit):
        return lax.ppermute(array, "tp", [(i, i ^ (1 << bit)) for i in range(self.count)])

    def reduce_scatter(self, parts):
        held = parts
        for bit in range(self.bits):
            half = held.shape[1] // 2
            received = self.swap(held[:, :half].astype(jnp.bfloat16), bit)
            held = held[:, half:].astype(jnp.float32) + received.astype(jnp.float32)
        return held

    def gather(self, own):
        held = own
        for bit in reversed(range(self.bits)):
            held = jnp.concatenate([held, self.swap(held, bit)], axis=1)
        return held


def softplus(v):
    return jnp.maximum(v, 0.0) + jnp.log1p(jnp.exp(-jnp.abs(v)))


def three(v, axis):
    high = v.astype(jnp.bfloat16)
    rest = v - high.astype(jnp.float32)
    mid = rest.astype(jnp.bfloat16)
    low = (rest - mid.astype(jnp.float32)).astype(jnp.bfloat16)
    return jnp.concatenate([high, mid, low], axis=axis)


def spread(v, width):
    heads = v.shape[1]
    high = v.astype(jnp.bfloat16)
    low = (v - high.astype(jnp.float32)).astype(jnp.bfloat16)
    row = lax.broadcasted_iota(jnp.int32, (2 * heads, heads * width), 0)
    column = lax.broadcasted_iota(jnp.int32, (2 * heads, heads * width), 1) // width
    pick = ((row == column) | (row - heads == column)).astype(jnp.float32).astype(jnp.bfloat16)
    return jnp.dot(
        jnp.concatenate([high, low], axis=1), pick, preferred_element_type=jnp.float32
    )


def decay_kernel(pre_r, add_r, rate_r, pre_c, add_c, rate_c, rows_ref, cols_ref, scale_ref, last_ref):
    two_h, length = pre_r.shape
    heads = two_h // 2
    width = scale_ref.shape[2] // heads
    at0 = lax.broadcasted_iota(jnp.int32, (length, length), 0)
    at1 = lax.broadcasted_iota(jnp.int32, (length, length), 1)
    lower = (at0 >= at1).astype(jnp.float32).astype(jnp.bfloat16)
    upper = (at0 <= at1).astype(jnp.float32).astype(jnp.bfloat16)

    dt_r = softplus(pre_r[...])
    log_r = add_r[...] - dt_r * jnp.exp(rate_r[...])
    sum_f = jnp.dot(three(log_r[:heads], 0), upper, preferred_element_type=jnp.float32)
    sum_b = jnp.dot(three(log_r[heads:], 0), lower, preferred_element_type=jnp.float32)
    run_f = sum_f[:heads] + sum_f[heads : 2 * heads] + sum_f[2 * heads :]
    run_b = sum_b[:heads] + sum_b[heads : 2 * heads] + sum_b[2 * heads :]
    rows_ref[0] = jnp.log(dt_r[:heads]) - run_f
    rows_ref[1] = jnp.log(dt_r[heads:]) - run_b
    rows_ref[2] = jnp.log(dt_r[:heads] + dt_r[heads:])

    dt_c = softplus(pre_c[...])
    log_c = add_c[...] - dt_c * jnp.exp(rate_c[...])
    col_f = jnp.dot(lower, three(log_c[:, :heads], 1), preferred_element_type=jnp.float32)
    col_b = jnp.dot(upper, three(log_c[:, heads:], 1), preferred_element_type=jnp.float32)
    down_f = col_f[:, :heads] + col_f[:, heads : 2 * heads] + col_f[:, 2 * heads :]
    down_b = col_b[:, :heads] + col_b[:, heads : 2 * heads] + col_b[:, 2 * heads :]
    cols_ref[0] = down_f
    cols_ref[1] = down_b
    end_f = down_f[length - 1 : length]
    end_b = down_b[0:1]
    scale_ref[0] = spread(jnp.exp(end_f - down_f) * dt_c[:, :heads], width)
    scale_ref[1] = spread(jnp.exp(end_b - down_b) * dt_c[:, heads:], width)
    last_ref[0] = spread(jnp.broadcast_to(jnp.exp(end_f), (8, heads)), width)
    last_ref[1] = spread(jnp.broadcast_to(jnp.exp(end_b), (8, heads)), width)


def state_kernel(values_ref, inputs_ref, scale_ref, last_ref, out_ref):
    groups = inputs_ref.shape[1] // STATE
    wide = values_ref.shape[1] // groups
    values = values_ref[...].astype(jnp.float32)
    for way in range(2):
        scaled = (values * scale_ref[way]).astype(jnp.bfloat16)
        for g in range(groups):
            out_ref[way, :STATE, g * wide : (g + 1) * wide] = lax.dot_general(
                inputs_ref[:, g * STATE : (g + 1) * STATE],
                scaled[:, g * wide : (g + 1) * wide],
                (((0,), (0,)), ((), ())),
                preferred_element_type=jnp.float32,
            )
        out_ref[way, STATE:, :] = jnp.concatenate([last_ref[way], last_ref[way]], axis=0)


def within_kernel(values_ref, inputs_ref, readout_ref, rows_ref, cols_ref, out_ref):
    heads = rows_ref.shape[1]
    length = values_ref.shape[0]
    width = values_ref.shape[1] // heads
    tile = min(256, length)
    groups = inputs_ref.shape[1] // STATE
    per_group = heads // groups
    pack = max(1, 128 // width)
    lane = lax.broadcasted_iota(jnp.int32, (length, pack * width), 1) // width
    at0 = lax.broadcasted_iota(jnp.int32, (tile, tile), 0)
    at1 = lax.broadcasted_iota(jnp.int32, (tile, tile), 1)
    for g in range(groups):
        for i in range(length // tile):
            here = slice(i * tile, (i + 1) * tile)
            scores = lax.dot_general(
                readout_ref[here, g * STATE : (g + 1) * STATE],
                inputs_ref[:, g * STATE : (g + 1) * STATE],
                (((1,), (1,)), ((), ())),
                preferred_element_type=jnp.float32,
            )
            for first in range(0, per_group, pack):
                total = None
                channels = slice((g * per_group + first) * width, (g * per_group + first + pack) * width)
                packed = values_ref[:, channels]
                for sub in range(pack):
                    h = g * per_group + first + sub
                    own = jnp.where(lane == sub, packed, jnp.zeros_like(packed))
                    down_f = cols_ref[0, here, h : h + 1]
                    down_b = cols_ref[1, here, h : h + 1]
                    pieces = []
                    for j in range(length // tile):
                        there = slice(j * tile, (j + 1) * tile)
                        if i > j:
                            gap = down_f + rows_ref[0, h : h + 1, there]
                        elif i < j:
                            gap = down_b + rows_ref[1, h : h + 1, there]
                        else:
                            gap = jnp.where(
                                at0 > at1,
                                down_f + rows_ref[0, h : h + 1, there],
                                jnp.where(
                                    at0 < at1,
                                    down_b + rows_ref[1, h : h + 1, there],
                                    rows_ref[2, h : h + 1, there],
                                ),
                            )
                        pieces.append((scores[:, there] * jnp.exp(gap)).astype(jnp.bfloat16))
                    weights = jnp.concatenate(pieces, axis=1)
                    term = jnp.dot(weights, own, preferred_element_type=jnp.float32)
                    total = term if total is None else total + term
                out_ref[here, channels] = total


def close_kernel(within_ref, readout_ref, cols_ref, states_ref, valve_ref, factor_ref, map_ref, out_ref):
    groups = readout_ref.shape[1] // STATE
    wide = within_ref.shape[1] // groups
    heads = cols_ref.shape[2]
    width = within_ref.shape[1] // heads
    length = within_ref.shape[0]
    lift_f = spread(jnp.exp(cols_ref[0]), width)
    lift_b = spread(jnp.exp(cols_ref[1]), width)
    blended = []
    for g in range(groups):
        at = slice(g * wide, (g + 1) * wide)
        readout = readout_ref[:, g * STATE : (g + 1) * STATE]
        carried_f = jnp.dot(readout, states_ref[0, :, at], preferred_element_type=jnp.float32)
        carried_b = jnp.dot(readout, states_ref[1, :, at], preferred_element_type=jnp.float32)
        mixed = within_ref[:, at] + carried_f * lift_f[:, at] + carried_b * lift_b[:, at]
        valve = valve_ref[:, at].astype(jnp.float32)
        gated = mixed * (valve / (1.0 + jnp.exp(-valve)))
        square = jnp.mean(gated * gated, axis=1, keepdims=True)
        scaled = gated * lax.rsqrt(square + EPSILON)
        blended.append((scaled * factor_ref[:, at]).astype(jnp.bfloat16))
    rows = jnp.concatenate(blended, axis=1)
    out_ref[...] = jnp.dot(rows, map_ref[...], preferred_element_type=jnp.float32).astype(jnp.bfloat16)


def conv_rows(padded, kernel, length):
    summed = padded[0:length] * kernel[0]
    for offset in range(1, kernel.shape[0]):
        summed = summed + padded[offset : offset + length] * kernel[offset]
    return summed


def halo(block, width):
    count = lax.axis_size("sp")
    forward = [(i, i + 1) for i in range(count - 1)]
    backward = [(b, a) for a, b in forward]
    low = lax.ppermute(block[block.shape[0] - width :], "sp", forward)
    high = lax.ppermute(block[:width], "sp", backward)
    return jnp.concatenate([low, block, high], axis=0)


def call(kernel, outs, *args):
    return pl.pallas_call(
        kernel,
        out_shape=[jax.ShapeDtypeStruct(shape, kind) for shape, kind in outs],
        compiler_params=pltpu.CompilerParams(vmem_limit_bytes=56 * 1024 * 1024),
        name=kernel.__name__,
    )(*args)


def solution(mesh):
    cycle = ring_cycle(mesh)
    sp_count = mesh.shape["sp"]
    tp_count = mesh.shape["tp"]
    place = {s: i for i, s in enumerate(cycle)}
    right = [(cycle[i], cycle[(i + 1) % sp_count]) for i in range(sp_count)]
    left = [(b, a) for a, b in right]
    tp = Butterfly(tp_count)
    scatter_place = np.argsort(np.array(tp.scatter_mask))
    gather_place = np.argsort(np.array(tp.gather_mask))

    def came_from(steps):
        table = [cycle[(place[s] - steps) % sp_count] for s in range(sp_count)]
        return jnp.asarray(np.array(table, np.int32))[lax.axis_index("sp")]

    def ring(upper, lower):
        join = jnp.concatenate([upper, lower], axis=0)
        half = upper.shape[0]
        yield came_from(0), upper, lower
        going, coming = join, join
        for step in range(1, (sp_count - 1) // 2 + 1):
            going = lax.ppermute(going, "sp", right)
            coming = lax.ppermute(coming, "sp", left)
            yield came_from(step), going[:half], going[half:]
            yield came_from(-step), coming[:half], coming[half:]
        if sp_count % 2 == 0:
            far = sp_count // 2
            yield came_from(far), lax.ppermute(going[:half], "sp", right), None
            yield came_from(far), None, lax.ppermute(coming[half:], "sp", left)

    def shards(
        skip_trunk_vector,
        valve_preactivation,
        projected_heads_payload,
        cluster_ingests,
        cluster_observers,
        pre_softplus_increments,
        attenuation_ln_rate,
        additional_attenuation,
        payload_conv_weights,
        ingest_conv_weights,
        observer_conv_weights,
        valved_cluster_factor,
        closing_map_matrix,
        dense_standardize_factor,
        dense_valve_map,
        dense_payload_map,
        valve_series_smoother,
        payload_series_smoother,
        dense_contract_map,
    ):
        length = skip_trunk_vector.shape[0]
        heads = pre_softplus_increments.shape[2]
        channels = projected_heads_payload.shape[1]
        in_cols = cluster_ingests.shape[1]
        own_cols = skip_trunk_vector.shape[1]
        me = lax.axis_index("tp")

        joined = jnp.concatenate([projected_heads_payload, cluster_ingests, cluster_observers], axis=1)
        taps = jnp.concatenate([payload_conv_weights, ingest_conv_weights, observer_conv_weights], axis=1)
        padded = halo(joined, taps.shape[0] // 2)

        full = own_cols * tp_count
        hidden_cols = dense_valve_map.shape[1]
        chunk = dense_valve_map.shape[0]

        def position(source, places):
            block = source * chunk // own_cols
            return jnp.asarray(places.astype(np.int32))[block ^ me] * own_cols + source * chunk % own_cols

        valve_full = jnp.zeros((full, hidden_cols), jnp.bfloat16)
        payload_full = jnp.zeros((full, hidden_cols), jnp.bfloat16)
        for source, valve_rows, payload_rows in ring(dense_valve_map, dense_payload_map):
            at = position(source, gather_place)
            if valve_rows is not None:
                valve_full = lax.dynamic_update_slice(valve_full, valve_rows, (at, 0))
            if payload_rows is not None:
                payload_full = lax.dynamic_update_slice(payload_full, payload_rows, (at, 0))
        contract_full = jnp.zeros((hidden_cols, full), jnp.bfloat16)
        middle_row = hidden_cols // 2
        for source, top, bottom in ring(dense_contract_map[:middle_row], dense_contract_map[middle_row:]):
            at = position(source, scatter_place)
            if top is not None:
                contract_full = lax.dynamic_update_slice(contract_full, top, (0, at))
            if bottom is not None:
                contract_full = lax.dynamic_update_slice(contract_full, bottom, (middle_row, at))

        closing = jnp.concatenate(
            [
                lax.dynamic_slice_in_dim(closing_map_matrix, (me ^ m) * own_cols, own_cols, axis=1)
                for m in tp.scatter_mask
            ],
            axis=1,
        )
        gain = jnp.concatenate(
            [
                lax.dynamic_slice_in_dim(dense_standardize_factor, (me ^ m) * own_cols, own_cols)
                for m in tp.gather_mask
            ]
        )

        def by_row(a):
            return jnp.transpose(a, (0, 2, 1)).reshape(2 * heads, length)

        def by_column(a):
            return jnp.transpose(a, (1, 0, 2)).reshape(length, 2 * heads)

        rate = attenuation_ln_rate.reshape(2 * heads)
        rows, cols, scale, last = call(
            decay_kernel,
            [
                ((3, heads, length), jnp.float32),
                ((2, length, heads), jnp.float32),
                ((2, length, channels), jnp.float32),
                ((2, 8, channels), jnp.float32),
            ],
            by_row(pre_softplus_increments),
            by_row(additional_attenuation),
            rate[:, None],
            by_column(pre_softplus_increments),
            by_column(additional_attenuation),
            rate[None, :],
        )

        convolved = jax.nn.silu(conv_rows(padded.astype(jnp.float32), taps, length)).astype(jnp.bfloat16)
        values = convolved[:, :channels]
        inputs = convolved[:, channels : channels + in_cols]
        readout = convolved[:, channels + in_cols :]
        (summary,) = call(
            state_kernel, [((2, STATE + TAIL, channels), jnp.float32)], values, inputs, scale, last
        )

        def carried(own, sign):
            state, decay = own[:STATE], own[STATE : STATE + 1]
            before, before_decay = jnp.zeros_like(state), jnp.ones_like(decay)
            offset = 1
            while offset < sp_count:
                high = decay.astype(jnp.bfloat16)
                low = (decay - high.astype(jnp.float32)).astype(jnp.bfloat16)
                tail = jnp.concatenate([high, low, jnp.zeros((TAIL - 2, channels), jnp.bfloat16)], axis=0)
                message = jnp.concatenate([state.astype(jnp.bfloat16), tail], axis=0)
                pairs = [(i, i + sign * offset) for i in range(sp_count) if 0 <= i + sign * offset < sp_count]
                received = lax.ppermute(message, "sp", pairs).astype(jnp.float32)
                got, got_decay = received[:STATE], received[STATE : STATE + 1] + received[STATE + 1 : STATE + 2]
                before = got * before_decay + before
                before_decay = before_decay * got_decay
                state = got * decay + state
                decay = decay * got_decay
                offset *= 2
            return before.astype(jnp.bfloat16)

        (within,) = call(
            within_kernel, [((length, channels), jnp.float32)], values, inputs, readout, rows, cols
        )
        states = jnp.stack([carried(summary[0], 1), carried(summary[1], -1)])
        (partial_out,) = call(
            close_kernel,
            [((length, full), jnp.bfloat16)],
            within,
            readout,
            cols,
            states,
            valve_preactivation,
            valved_cluster_factor[None, :],
            closing,
        )
        projected = tp.reduce_scatter(partial_out)
        middle = (skip_trunk_vector.astype(jnp.float32) + projected).astype(jnp.bfloat16)
        middle_all = tp.gather(middle).astype(jnp.float32)
        square = jnp.mean(middle_all * middle_all, axis=1, keepdims=True)
        normed = (middle_all * lax.rsqrt(square + EPSILON) * gain).astype(jnp.bfloat16)
        gate_rows = jnp.dot(normed, valve_full, preferred_element_type=jnp.float32).astype(jnp.bfloat16)
        value_rows = jnp.dot(normed, payload_full, preferred_element_type=jnp.float32).astype(jnp.bfloat16)
        up_padded = halo(jnp.concatenate([gate_rows, value_rows], axis=1), valve_series_smoother.shape[0] // 2)
        taps_both = jnp.concatenate([valve_series_smoother, payload_series_smoother], axis=1)
        smoothed = conv_rows(up_padded.astype(jnp.float32), taps_both, length)
        hidden = (jax.nn.silu(smoothed[:, :hidden_cols]) * smoothed[:, hidden_cols:]).astype(jnp.bfloat16)
        partial_down = jnp.dot(hidden, contract_full, preferred_element_type=jnp.float32)
        down_sum = tp.reduce_scatter(partial_down.astype(jnp.bfloat16))
        return (middle.astype(jnp.float32) + down_sum).astype(jnp.bfloat16)

    return jax.shard_map(
        shards,
        mesh=mesh,
        in_specs=(
            P("sp", "tp"),
            P("sp", "tp"),
            P("sp", "tp"),
            P("sp", "tp"),
            P("sp", "tp"),
            P(None, "sp", "tp"),
            P(None, "tp"),
            P(None, "sp", "tp"),
            P(None, "tp"),
            P(None, "tp"),
            P(None, "tp"),
            P("tp"),
            P("tp", None),
            P(),
            P("sp", "tp"),
            P("sp", "tp"),
            P(None, "tp"),
            P(None, "tp"),
            P("tp", "sp"),
        ),
        out_specs=P("sp", "tp"),
        check_vma=False,
    )
```

```python
import functools

import jax
import jax.numpy as jnp
import numpy as np
from jax import lax
from jax.experimental import pallas as pl
from jax.experimental.pallas import tpu as pltpu
from jax.sharding import PartitionSpec as P


STATE = 128
EPSILON = 1e-06
TAIL = 16


def ring_cycle(mesh):
    line = mesh.devices[:, 0].ravel()
    count = len(line)
    if not all(hasattr(d, "coords") for d in line):
        return list(range(count))
    spots = {(d.coords[2], d.coords[1]): i for i, d in enumerate(line)}
    deep = sorted({z for z, _ in spots})
    wide = sorted({y for _, y in spots})
    if len(spots) != count or len(deep) % 2 or len(wide) < 2:
        return list(range(count))
    path = []
    for at, z in enumerate(deep):
        row = wide[1:] if at % 2 == 0 else wide[:0:-1]
        path += [(z, y) for y in row]
    path += [(z, wide[0]) for z in reversed(deep)]
    return [spots[spot] for spot in path]


def bit_reverse(value, bits):
    return int(format(value, f"0{bits}b")[::-1], 2) if bits else 0


class Butterfly:
    def __init__(self, count):
        self.count = count
        self.bits = count.bit_length() - 1
        self.scatter_mask = [bit_reverse(count - 1 - p, self.bits) for p in range(count)]
        self.gather_mask = [bit_reverse(p, self.bits) for p in range(count)]

    def swap(self, array, bit):
        return lax.ppermute(array, "tp", [(i, i ^ (1 << bit)) for i in range(self.count)])

    def reduce_scatter(self, send, keep):
        for bit in range(self.bits):
            received = self.swap(send.astype(jnp.bfloat16), bit)
            held = keep.astype(jnp.float32) + received.astype(jnp.float32)
            half = held.shape[1] // 2
            send, keep = held[:, :half], held[:, half:]
        return held

    def gather(self, own):
        pieces = [own]
        for bit in reversed(range(self.bits)):
            held = pieces[0] if len(pieces) == 1 else jnp.concatenate(pieces, axis=1)
            pieces.append(self.swap(held, bit))
        return pieces


def softplus(v):
    return jnp.maximum(v, 0.0) + jnp.log1p(jnp.exp(-jnp.abs(v)))


def three(v, axis):
    high = v.astype(jnp.bfloat16)
    rest = v - high.astype(jnp.float32)
    mid = rest.astype(jnp.bfloat16)
    low = (rest - mid.astype(jnp.float32)).astype(jnp.bfloat16)
    return jnp.concatenate([high, mid, low], axis=axis)


def spread(v, width):
    heads = v.shape[1]
    high = v.astype(jnp.bfloat16)
    low = (v - high.astype(jnp.float32)).astype(jnp.bfloat16)
    row = lax.broadcasted_iota(jnp.int32, (2 * heads, heads * width), 0)
    column = lax.broadcasted_iota(jnp.int32, (2 * heads, heads * width), 1) // width
    pick = ((row == column) | (row - heads == column)).astype(jnp.float32).astype(jnp.bfloat16)
    return jnp.dot(
        jnp.concatenate([high, low], axis=1), pick, preferred_element_type=jnp.float32
    )


def decay_kernel(pre_ref, add_ref, rate_ref, rows_ref, cols_ref, scale_ref, last_ref):
    _, heads, length = pre_ref.shape
    width = scale_ref.shape[2] // heads
    at0 = lax.broadcasted_iota(jnp.int32, (length, length), 0)
    at1 = lax.broadcasted_iota(jnp.int32, (length, length), 1)
    steps, runs = [], []
    for way in range(2):
        reach = (at0 <= at1) if way == 0 else (at0 >= at1)
        reach = reach.astype(jnp.float32).astype(jnp.bfloat16)
        step = softplus(pre_ref[way])
        log = add_ref[way] - step * jnp.exp(rate_ref[:, way : way + 1])
        sums = jnp.dot(three(log, 0), reach, preferred_element_type=jnp.float32)
        run = sums[:heads] + sums[heads : 2 * heads] + sums[2 * heads :]
        rows_ref[way] = jnp.log(step) - run
        steps.append(step)
        runs.append(run)
    rows_ref[2] = jnp.log(steps[0] + steps[1])
    rest = jnp.zeros((128 - 4 * heads, length), jnp.float32)
    turned = jnp.concatenate([*runs, *steps, rest], axis=0).T
    for way in range(2):
        down = turned[:, way * heads : (way + 1) * heads]
        step = turned[:, (2 + way) * heads : (3 + way) * heads]
        end = down[length - 1 : length] if way == 0 else down[0:1]
        cols_ref[way] = down
        scale_ref[way] = spread(jnp.exp(end - down) * step, width)
        last_ref[way] = spread(jnp.broadcast_to(jnp.exp(end), (8, heads)), width)


def message(state, decay):
    high = decay.astype(jnp.bfloat16).astype(jnp.float32)
    low = decay - high
    row = lax.broadcasted_iota(jnp.int32, (TAIL, state.shape[1]), 0)
    tail = jnp.where(row == 0, high, jnp.where(row == 1, low, 0.0))
    return jnp.concatenate([state, tail], axis=0).astype(jnp.bfloat16)


def state_kernel(values_ref, inputs_ref, scale_ref, last_ref, window_ref, decay_ref, send_f_ref, send_b_ref):
    groups = inputs_ref.shape[1] // STATE
    wide = values_ref.shape[1] // groups
    values = values_ref[...].astype(jnp.float32)
    for way, send_ref in enumerate((send_f_ref, send_b_ref)):
        scaled = (values * scale_ref[way]).astype(jnp.bfloat16)
        state = jnp.concatenate(
            [
                lax.dot_general(
                    inputs_ref[:, g * STATE : (g + 1) * STATE],
                    scaled[:, g * wide : (g + 1) * wide],
                    (((0,), (0,)), ((), ())),
                    preferred_element_type=jnp.float32,
                )
                for g in range(groups)
            ],
            axis=1,
        )
        window_ref[way] = state
        decay_ref[way] = last_ref[way]
        send_ref[...] = message(state, last_ref[way, 0:1])


def link_kernel(first, final, *refs):
    got_refs, window_ref, decay_ref = refs[:2], refs[2], refs[3]
    before_ref, before_decay_ref = (None, None) if first else refs[4:6]
    outs = refs[4:] if first else refs[6:]
    for way in range(2):
        got = got_refs[way][:STATE].astype(jnp.float32)
        got_decay = got_refs[way][STATE : STATE + 1].astype(jnp.float32) + got_refs[way][
            STATE + 1 : STATE + 2
        ].astype(jnp.float32)
        before, before_decay = got, got_decay
        if not first:
            before = got * before_decay_ref[way, 0:1] + before_ref[way]
            before_decay = got_decay * before_decay_ref[way, 0:1]
        if final:
            outs[0][way] = before.astype(jnp.bfloat16)
            continue
        decay = decay_ref[way, 0:1]
        state = got * decay + window_ref[way]
        decay = decay * got_decay
        outs[0][way] = before
        outs[1][way] = jnp.broadcast_to(before_decay, outs[1].shape[1:])
        outs[2][way] = state
        outs[3][way] = jnp.broadcast_to(decay, outs[3].shape[1:])
        outs[4 + way][...] = message(state, decay)


def within_kernel(values_ref, inputs_ref, readout_ref, rows_ref, cols_ref, out_ref):
    heads = rows_ref.shape[1]
    length = values_ref.shape[0]
    width = values_ref.shape[1] // heads
    tile = min(256, length)
    groups = inputs_ref.shape[1] // STATE
    per_group = heads // groups
    pack = max(1, 128 // width)
    lane = lax.broadcasted_iota(jnp.int32, (length, pack * width), 1) // width
    at0 = lax.broadcasted_iota(jnp.int32, (tile, tile), 0)
    at1 = lax.broadcasted_iota(jnp.int32, (tile, tile), 1)
    for g in range(groups):
        for i in range(length // tile):
            here = slice(i * tile, (i + 1) * tile)
            scores = lax.dot_general(
                readout_ref[here, g * STATE : (g + 1) * STATE],
                inputs_ref[:, g * STATE : (g + 1) * STATE],
                (((1,), (1,)), ((), ())),
                preferred_element_type=jnp.float32,
            )
            for first in range(0, per_group, pack):
                total = None
                channels = slice((g * per_group + first) * width, (g * per_group + first + pack) * width)
                packed = values_ref[:, channels]
                for sub in range(pack):
                    h = g * per_group + first + sub
                    own = jnp.where(lane == sub, packed, jnp.zeros_like(packed))
                    down_f = cols_ref[0, here, h : h + 1]
                    down_b = cols_ref[1, here, h : h + 1]
                    pieces = []
                    for j in range(length // tile):
                        there = slice(j * tile, (j + 1) * tile)
                        if i > j:
                            gap = down_f + rows_ref[0, h : h + 1, there]
                        elif i < j:
                            gap = down_b + rows_ref[1, h : h + 1, there]
                        else:
                            gap = jnp.where(
                                at0 > at1,
                                down_f + rows_ref[0, h : h + 1, there],
                                jnp.where(
                                    at0 < at1,
                                    down_b + rows_ref[1, h : h + 1, there],
                                    rows_ref[2, h : h + 1, there],
                                ),
                            )
                        pieces.append((scores[:, there] * jnp.exp(gap)).astype(jnp.bfloat16))
                    weights = jnp.concatenate(pieces, axis=1)
                    term = jnp.dot(weights, own, preferred_element_type=jnp.float32)
                    total = term if total is None else total + term
                out_ref[here, channels] = total


def close_kernel(sizes, info_ref, within_ref, readout_ref, cols_ref, states_ref, valve_ref, factor_ref, map_ref, send_ref, keep_ref):
    groups = readout_ref.shape[1] // STATE
    wide = within_ref.shape[1] // groups
    heads = cols_ref.shape[2]
    width = within_ref.shape[1] // heads
    lift_f = spread(jnp.exp(cols_ref[0]), width)
    lift_b = spread(jnp.exp(cols_ref[1]), width)
    blended = []
    for g in range(groups):
        at = slice(g * wide, (g + 1) * wide)
        readout = readout_ref[:, g * STATE : (g + 1) * STATE]
        carried_f = jnp.dot(readout, states_ref[0, :, at], preferred_element_type=jnp.float32)
        carried_b = jnp.dot(readout, states_ref[1, :, at], preferred_element_type=jnp.float32)
        mixed = within_ref[:, at] + carried_f * lift_f[:, at] + carried_b * lift_b[:, at]
        valve = valve_ref[:, at].astype(jnp.float32)
        gated = mixed * (valve / (1.0 + jnp.exp(-valve)))
        square = jnp.mean(gated * gated, axis=1, keepdims=True)
        scaled = gated * lax.rsqrt(square + EPSILON)
        blended.append((scaled * factor_ref[:, at]).astype(jnp.bfloat16))
    rows = jnp.concatenate(blended, axis=1)
    sp_count, count = sizes
    block = map_ref.shape[1] // count
    for p in range(count):
        columns = pl.ds(pl.multiple_of(info_ref[2 * sp_count + p] * block, block), block)
        term = jnp.dot(rows, map_ref[:, columns], preferred_element_type=jnp.float32).astype(jnp.bfloat16)
        target, at = (send_ref, p) if p < count // 2 else (keep_ref, p - count // 2)
        target[:, at * block : (at + 1) * block] = term


def up_kernel(sizes, plan, counts, *refs):
    n_pieces, n_arrays = counts
    sp_count, tp_count = sizes
    info_ref, gain_ref = refs[:2]
    pieces = refs[2 : 2 + n_pieces]
    arrays = refs[2 + n_pieces : 2 + n_pieces + n_arrays]
    outs = refs[2 + n_pieces + n_arrays : 4 + n_pieces + n_arrays]
    rows_scr, gain_scr = refs[4 + n_pieces + n_arrays :]
    length, full = pieces[0].shape[0], gain_ref.shape[1]
    chunk, block = full // sp_count, full // tp_count
    for p in range(tp_count):
        at = pl.multiple_of(info_ref[2 * sp_count + tp_count + p] * block, block)
        gain_scr[:, p * block : (p + 1) * block] = gain_ref[:, pl.ds(at, block)]

    band = 64

    def norm(r, carry):
        rows = pl.ds(pl.multiple_of(r * band, band), band)
        parts = [piece[rows, :].astype(jnp.float32) for piece in pieces]
        square = sum(jnp.sum(part * part, axis=1, keepdims=True) for part in parts) / full
        factor = lax.rsqrt(square + EPSILON)
        start = 0
        for part in parts:
            for first in range(0, part.shape[1], chunk):
                at = start + first
                rows_scr[at // chunk, rows, :] = (
                    part[:, first : first + chunk] * factor * gain_scr[:, at : at + chunk]
                ).astype(jnp.bfloat16)
            start += part.shape[1]
        return carry

    lax.fori_loop(0, length // band, norm, 0)
    columns = outs[0].shape[1]
    tile = 256 if columns % 256 == 0 else columns
    for which in range(2):
        for j in range(columns // tile):
            at = slice(j * tile, (j + 1) * tile)
            total = None
            for array, first, source in plan[which]:
                term = jnp.dot(
                    rows_scr[info_ref[source] // chunk],
                    arrays[array][first : first + chunk, at],
                    preferred_element_type=jnp.float32,
                )
                total = term if total is None else total + term
            outs[which][:, at] = total.astype(jnp.bfloat16)


def down_kernel(sizes, plan, n_arrays, *refs):
    info_ref, hidden_ref = refs[:2]
    arrays = refs[2 : 2 + n_arrays]
    send_ref, keep_ref = refs[2 + n_arrays :]
    half = send_ref.shape[1]
    for source, parts in enumerate(plan):
        term = None
        for array, row in parts:
            depth, chunk = arrays[array].shape
            part = jnp.dot(
                hidden_ref[:, row : row + depth], arrays[array][...], preferred_element_type=jnp.float32
            )
            term = part if term is None else term + part
        term = term.astype(jnp.bfloat16)
        if len(plan) == 1:
            send_ref[...] = term[:, :half]
            keep_ref[...] = term[:, half:]
            continue
        at = info_ref[sizes[0] + source]

        @pl.when(at < half)
        def _():
            send_ref[:, pl.ds(pl.multiple_of(at, chunk), chunk)] = term

        @pl.when(at >= half)
        def _():
            keep_ref[:, pl.ds(pl.multiple_of(at - half, chunk), chunk)] = term


def conv_rows(padded, kernel, length):
    summed = padded[0:length] * kernel[0]
    for offset in range(1, kernel.shape[0]):
        summed = summed + padded[offset : offset + length] * kernel[offset]
    return summed


def edges(last, first):
    count = lax.axis_size("sp")
    forward = [(i, i + 1) for i in range(count - 1)]
    backward = [(b, a) for a, b in forward]
    low = lax.ppermute(last, "sp", forward)
    high = lax.ppermute(first, "sp", backward)
    return low, high


def call(kernel, outs, *args, scalars=0, scratch=()):
    spaces = [pltpu.SMEM] * scalars + [pltpu.VMEM] * (len(args) - scalars)
    return pl.pallas_call(
        kernel,
        out_shape=[jax.ShapeDtypeStruct(shape, kind) for shape, kind in outs],
        in_specs=[pl.BlockSpec(memory_space=space) for space in spaces],
        scratch_shapes=list(scratch),
        compiler_params=pltpu.CompilerParams(vmem_limit_bytes=32 * 1024 * 1024),
    )(*args)


def solution(mesh):
    cycle = ring_cycle(mesh)
    sp_count = mesh.shape["sp"]
    tp_count = mesh.shape["tp"]
    place = {s: i for i, s in enumerate(cycle)}
    right = [(cycle[i], cycle[(i + 1) % sp_count]) for i in range(sp_count)]
    left = [(b, a) for a, b in right]
    tp = Butterfly(tp_count)
    scatter_place = np.argsort(np.array(tp.scatter_mask))
    gather_place = np.argsort(np.array(tp.gather_mask))

    def table(chunk, own_cols):
        lines = []
        for s in range(sp_count):
            for t in range(tp_count):
                up, down = [], []
                for steps in range(sp_count):
                    block, rest = divmod(cycle[(place[s] - steps) % sp_count] * chunk, own_cols)
                    up.append(gather_place[block ^ t] * own_cols + rest)
                    down.append(scatter_place[block ^ t] * own_cols + rest)
                lines.append(up + down + [t ^ m for m in tp.scatter_mask] + [t ^ m for m in tp.gather_mask])
        return np.array(lines, np.int32)

    def send_on(array, pairs):
        return lax.ppermute(array, "sp", pairs)

    def ring(join, half):
        out = []
        going, coming = join, join
        for step in range(1, (sp_count - 1) // 2 + 1):
            going = send_on(going, right)
            coming = send_on(coming, left)
            out += [(step, going, None), (-step, coming, None)]
        if sp_count % 2 == 0:
            far = sp_count // 2
            out.append((far, send_on(going[:half], right), 0))
            out.append((far, send_on(coming[half:], left), 1))
        return out

    def shards(
        skip_trunk_vector,
        valve_preactivation,
        projected_heads_payload,
        cluster_ingests,
        cluster_observers,
        pre_softplus_increments,
        attenuation_ln_rate,
        additional_attenuation,
        payload_conv_weights,
        ingest_conv_weights,
        observer_conv_weights,
        valved_cluster_factor,
        closing_map_matrix,
        dense_standardize_factor,
        dense_valve_map,
        dense_payload_map,
        valve_series_smoother,
        payload_series_smoother,
        dense_contract_map,
    ):
        length = skip_trunk_vector.shape[0]
        heads = pre_softplus_increments.shape[2]
        channels = projected_heads_payload.shape[1]
        in_cols = cluster_ingests.shape[1]
        own_cols = skip_trunk_vector.shape[1]
        me = lax.axis_index("tp")

        margin = payload_conv_weights.shape[0] // 2
        streams = (projected_heads_payload, cluster_ingests, cluster_observers)
        low, high = edges(
            jnp.concatenate([a[length - margin :] for a in streams], axis=1),
            jnp.concatenate([a[:margin] for a in streams], axis=1),
        )

        full = own_cols * tp_count
        hidden_cols = dense_valve_map.shape[1]
        chunk = dense_valve_map.shape[0]
        middle_row = hidden_cols // 2
        up_ring = [(0, dense_valve_map, 0), (0, dense_payload_map, 1)]
        up_ring += ring(jnp.concatenate([dense_valve_map, dense_payload_map], axis=0), chunk)
        down_ring = [(0, dense_contract_map, None)] + ring(dense_contract_map, middle_row)

        info = jnp.asarray(table(chunk, own_cols))[lax.axis_index("sp") * tp_count + me]

        rows, cols, scale, last = call(
            decay_kernel,
            [
                ((3, heads, length), jnp.float32),
                ((2, length, heads), jnp.float32),
                ((2, length, channels), jnp.float32),
                ((2, 8, channels), jnp.float32),
            ],
            jnp.transpose(pre_softplus_increments, (0, 2, 1)),
            jnp.transpose(additional_attenuation, (0, 2, 1)),
            attenuation_ln_rate.T,
        )

        def mixed(array, low, high, kernel):
            padded = jnp.concatenate([low, array, high], axis=0).astype(jnp.float32)
            return jax.nn.silu(conv_rows(padded, kernel, length)).astype(jnp.bfloat16)

        ends = (channels, channels + in_cols)
        lows, highs = jnp.split(low, ends, axis=1), jnp.split(high, ends, axis=1)
        values = mixed(projected_heads_payload, lows[0], highs[0], payload_conv_weights)
        inputs = mixed(cluster_ingests, lows[1], highs[1], ingest_conv_weights)
        readout = mixed(cluster_observers, lows[2], highs[2], observer_conv_weights)
        wide_state = ((2, STATE, channels), jnp.float32)
        wide_decay = ((2, 8, channels), jnp.float32)
        sent = ((STATE + TAIL, channels), jnp.bfloat16)
        window, decay, send_f, send_b = call(
            state_kernel, [wide_state, wide_decay, sent, sent], values, inputs, scale, last
        )
        (within,) = call(
            within_kernel, [((length, channels), jnp.float32)], values, inputs, readout, rows, cols
        )

        before, offset = (), 1
        while offset < sp_count:
            forward = [(i, i + offset) for i in range(sp_count - offset)]
            got_f = lax.ppermute(send_f, "sp", forward)
            got_b = lax.ppermute(send_b, "sp", [(b, a) for a, b in forward])
            final = 2 * offset >= sp_count
            outs = [((2, STATE, channels), jnp.bfloat16)]
            if not final:
                outs = [wide_state, wide_decay, wide_state, wide_decay, sent, sent]
            result = call(
                functools.partial(link_kernel, offset == 1, final), outs, got_f, got_b, window, decay, *before
            )
            if final:
                states = result[0]
            else:
                before, (window, decay, send_f, send_b) = tuple(result[:2]), result[2:]
            offset *= 2

        half_full = full // 2
        send, keep = call(
            functools.partial(close_kernel, (sp_count, tp_count)),
            [((length, half_full), jnp.bfloat16)] * 2,
            info,
            within,
            readout,
            cols,
            states,
            valve_preactivation,
            valved_cluster_factor[None, :],
            closing_map_matrix,
            scalars=1,
        )
        projected = tp.reduce_scatter(send, keep)
        middle = (skip_trunk_vector.astype(jnp.float32) + projected).astype(jnp.bfloat16)
        pieces = tp.gather(middle)

        arrays, plan = [], ([], [])
        for steps, array, part in up_ring:
            for which in (0, 1) if part is None else (part,):
                plan[which].append((len(arrays), which * chunk if part is None else 0, steps % sp_count))
            arrays.append(array)
        gate_rows, value_rows = call(
            functools.partial(up_kernel, (sp_count, tp_count), plan, (len(pieces), len(arrays))),
            [((length, hidden_cols), jnp.bfloat16)] * 2,
            info,
            dense_standardize_factor[None, :],
            *pieces,
            *arrays,
            scalars=1,
            scratch=[pltpu.VMEM((sp_count, length, chunk), jnp.bfloat16), pltpu.VMEM((1, full), jnp.float32)],
        )
        margin = valve_series_smoother.shape[0] // 2
        low, high = edges(
            jnp.concatenate([gate_rows[length - margin :], value_rows[length - margin :]], axis=1),
            jnp.concatenate([gate_rows[:margin], value_rows[:margin]], axis=1),
        )

        def smooth(array, low, high, kernel):
            return conv_rows(jnp.concatenate([low, array, high], axis=0).astype(jnp.float32), kernel, length)

        gate = smooth(gate_rows, low[:, :hidden_cols], high[:, :hidden_cols], valve_series_smoother)
        value = smooth(value_rows, low[:, hidden_cols:], high[:, hidden_cols:], payload_series_smoother)
        hidden = (jax.nn.silu(gate) * value).astype(jnp.bfloat16)

        arrays = []
        if chunk % 128 == 0:
            plan = [[] for _ in range(sp_count)]
            for steps, array, part in down_ring:
                plan[steps % sp_count].append((len(arrays), middle_row if part == 1 else 0))
                arrays.append(array)
        else:
            whole = jnp.zeros((hidden_cols, full), jnp.bfloat16)
            for steps, array, part in down_ring:
                corner = (middle_row if part == 1 else 0, info[sp_count + steps % sp_count])
                whole = lax.dynamic_update_slice(whole, array, corner)
            arrays, plan = [whole], [[(0, 0)]]
        send, keep = call(
            functools.partial(down_kernel, (sp_count, tp_count), plan, len(arrays)),
            [((length, half_full), jnp.bfloat16)] * 2,
            info,
            hidden,
            *arrays,
            scalars=1,
        )
        down_sum = tp.reduce_scatter(send, keep)
        return (middle.astype(jnp.float32) + down_sum).astype(jnp.bfloat16)

    return jax.shard_map(
        shards,
        mesh=mesh,
        in_specs=(
            P("sp", "tp"),
            P("sp", "tp"),
            P("sp", "tp"),
            P("sp", "tp"),
            P("sp", "tp"),
            P(None, "sp", "tp"),
            P(None, "tp"),
            P(None, "sp", "tp"),
            P(None, "tp"),
            P(None, "tp"),
            P(None, "tp"),
            P("tp"),
            P("tp", None),
            P(),
            P("sp", "tp"),
            P("sp", "tp"),
            P(None, "tp"),
            P(None, "tp"),
            P("tp", "sp"),
        ),
        out_specs=P("sp", "tp"),
        check_vma=False,
    )
```

```python
import functools

import jax
import jax.numpy as jnp
import numpy as np
from jax import lax
from jax.experimental import pallas as pl
from jax.experimental.pallas import tpu as pltpu
from jax.sharding import PartitionSpec as P


STATE = 128
EPSILON = 1e-06
TAIL = 16
LIMIT = 16


def ring_cycle(mesh):
    line = mesh.devices[:, 0].ravel()
    count = len(line)
    if not all(hasattr(d, "coords") for d in line):
        return list(range(count))
    spots = {(d.coords[2], d.coords[1]): i for i, d in enumerate(line)}
    deep = sorted({z for z, _ in spots})
    wide = sorted({y for _, y in spots})
    if len(spots) != count or len(deep) % 2 or len(wide) < 2:
        return list(range(count))
    path = []
    for at, z in enumerate(deep):
        row = wide[1:] if at % 2 == 0 else wide[:0:-1]
        path += [(z, y) for y in row]
    path += [(z, wide[0]) for z in reversed(deep)]
    return [spots[spot] for spot in path]


def bit_reverse(value, bits):
    return int(format(value, f"0{bits}b")[::-1], 2) if bits else 0


class Butterfly:
    def __init__(self, count):
        self.count = count
        self.bits = count.bit_length() - 1
        self.scatter_mask = [bit_reverse(count - 1 - p, self.bits) for p in range(count)]
        self.gather_mask = [bit_reverse(p, self.bits) for p in range(count)]

    def swap(self, array, bit):
        return lax.ppermute(array, "tp", [(i, i ^ (1 << bit)) for i in range(self.count)])

    def reduce_scatter(self, send, keep):
        for bit in range(self.bits):
            received = self.swap(send.astype(jnp.bfloat16), bit)
            held = keep.astype(jnp.float32) + received.astype(jnp.float32)
            half = held.shape[1] // 2
            send, keep = held[:, :half], held[:, half:]
        return held

    def gather(self, own):
        pieces = [own]
        for bit in reversed(range(self.bits)):
            held = pieces[0] if len(pieces) == 1 else jnp.concatenate(pieces, axis=1)
            pieces.append(self.swap(held, bit))
        return pieces


def softplus(v):
    return jnp.maximum(v, 0.0) + jnp.log1p(jnp.exp(-jnp.abs(v)))


def three(v, axis):
    high = v.astype(jnp.bfloat16)
    rest = v - high.astype(jnp.float32)
    mid = rest.astype(jnp.bfloat16)
    low = (rest - mid.astype(jnp.float32)).astype(jnp.bfloat16)
    return jnp.concatenate([high, mid, low], axis=axis)


def spread(v, width):
    heads = v.shape[1]
    high = v.astype(jnp.bfloat16)
    low = (v - high.astype(jnp.float32)).astype(jnp.bfloat16)
    row = lax.broadcasted_iota(jnp.int32, (2 * heads, heads * width), 0)
    column = lax.broadcasted_iota(jnp.int32, (2 * heads, heads * width), 1) // width
    pick = ((row == column) | (row - heads == column)).astype(jnp.float32).astype(jnp.bfloat16)
    return jnp.dot(
        jnp.concatenate([high, low], axis=1), pick, preferred_element_type=jnp.float32
    )


def decay_kernel(pre_ref, add_ref, rate_ref, rows_ref, cols_ref, scale_ref, last_ref):
    _, heads, length = pre_ref.shape
    width = scale_ref.shape[2] // heads
    at0 = lax.broadcasted_iota(jnp.int32, (length, length), 0)
    at1 = lax.broadcasted_iota(jnp.int32, (length, length), 1)
    steps, runs = [], []
    for way in range(2):
        reach = (at0 <= at1) if way == 0 else (at0 >= at1)
        reach = reach.astype(jnp.float32).astype(jnp.bfloat16)
        step = softplus(pre_ref[way])
        log = add_ref[way] - step * jnp.exp(rate_ref[:, way : way + 1])
        sums = jnp.dot(three(log, 0), reach, preferred_element_type=jnp.float32)
        run = sums[:heads] + sums[heads : 2 * heads] + sums[2 * heads :]
        rows_ref[way] = jnp.log(step) - run
        steps.append(step)
        runs.append(run)
    rows_ref[2] = jnp.log(steps[0] + steps[1])
    rest = jnp.zeros((128 - 4 * heads, length), jnp.float32)
    turned = jnp.concatenate([*runs, *steps, rest], axis=0).T
    for way in range(2):
        down = turned[:, way * heads : (way + 1) * heads]
        step = turned[:, (2 + way) * heads : (3 + way) * heads]
        end = down[length - 1 : length] if way == 0 else down[0:1]
        cols_ref[way] = down
        scale_ref[way] = spread(jnp.exp(end - down) * step, width)
        last_ref[way] = spread(jnp.broadcast_to(jnp.exp(end), (8, heads)), width)


def message(state, decay):
    high = decay.astype(jnp.bfloat16).astype(jnp.float32)
    low = decay - high
    row = lax.broadcasted_iota(jnp.int32, (TAIL, state.shape[1]), 0)
    tail = jnp.where(row == 0, high, jnp.where(row == 1, low, 0.0))
    return jnp.concatenate([state, tail], axis=0).astype(jnp.bfloat16)


def state_kernel(values_ref, inputs_ref, scale_ref, last_ref, window_ref, send_f_ref, send_b_ref):
    groups = inputs_ref.shape[1] // STATE
    wide = values_ref.shape[1] // groups
    values = values_ref[...].astype(jnp.float32)
    for way, send_ref in enumerate((send_f_ref, send_b_ref)):
        scaled = (values * scale_ref[way]).astype(jnp.bfloat16)
        state = jnp.concatenate(
            [
                lax.dot_general(
                    inputs_ref[:, g * STATE : (g + 1) * STATE],
                    scaled[:, g * wide : (g + 1) * wide],
                    (((0,), (0,)), ((), ())),
                    preferred_element_type=jnp.float32,
                )
                for g in range(groups)
            ],
            axis=1,
        )
        window_ref[way, :STATE] = state
        window_ref[way, STATE:] = last_ref[way]
        send_ref[...] = message(state, last_ref[way, 0:1])


def link_kernel(first, final, *refs):
    got_refs, refs = refs[:2], list(refs[2:])
    before_ref = None if first else refs.pop(0)
    window_ref = None if final else refs.pop(0)
    for way in range(2):
        got = got_refs[way][:STATE].astype(jnp.float32)
        got_decay = got_refs[way][STATE : STATE + 1].astype(jnp.float32) + got_refs[way][
            STATE + 1 : STATE + 2
        ].astype(jnp.float32)
        before, before_decay = got, got_decay
        if not first:
            held_decay = before_ref[way, STATE : STATE + 1]
            before = got * held_decay + before_ref[way, :STATE]
            before_decay = got_decay * held_decay
        if final:
            refs[0][way] = before.astype(jnp.bfloat16)
            continue
        decay = window_ref[way, STATE : STATE + 1]
        state = got * decay + window_ref[way, :STATE]
        decay = decay * got_decay
        for ref, value, factor in ((refs[0], before, before_decay), (refs[1], state, decay)):
            ref[way, :STATE] = value
            ref[way, STATE:] = jnp.broadcast_to(factor, (8, factor.shape[1]))
        refs[2 + way][...] = message(state, decay)


def within_kernel(values_ref, inputs_ref, readout_ref, rows_ref, cols_ref, out_ref):
    heads = rows_ref.shape[1]
    length = values_ref.shape[0]
    width = values_ref.shape[1] // heads
    tile = min(256, length)
    groups = inputs_ref.shape[1] // STATE
    per_group = heads // groups
    pack = max(1, 128 // width)
    lane = lax.broadcasted_iota(jnp.int32, (length, pack * width), 1) // width
    at0 = lax.broadcasted_iota(jnp.int32, (tile, tile), 0)
    at1 = lax.broadcasted_iota(jnp.int32, (tile, tile), 1)
    for g in range(groups):
        for i in range(length // tile):
            here = slice(i * tile, (i + 1) * tile)
            scores = lax.dot_general(
                readout_ref[here, g * STATE : (g + 1) * STATE],
                inputs_ref[:, g * STATE : (g + 1) * STATE],
                (((1,), (1,)), ((), ())),
                preferred_element_type=jnp.float32,
            )
            for first in range(0, per_group, pack):
                total = None
                channels = slice((g * per_group + first) * width, (g * per_group + first + pack) * width)
                packed = values_ref[:, channels]
                for sub in range(pack):
                    h = g * per_group + first + sub
                    own = jnp.where(lane == sub, packed, jnp.zeros_like(packed))
                    down_f = cols_ref[0, here, h : h + 1]
                    down_b = cols_ref[1, here, h : h + 1]
                    pieces = []
                    for j in range(length // tile):
                        there = slice(j * tile, (j + 1) * tile)
                        if i > j:
                            gap = down_f + rows_ref[0, h : h + 1, there]
                        elif i < j:
                            gap = down_b + rows_ref[1, h : h + 1, there]
                        else:
                            gap = jnp.where(
                                at0 > at1,
                                down_f + rows_ref[0, h : h + 1, there],
                                jnp.where(
                                    at0 < at1,
                                    down_b + rows_ref[1, h : h + 1, there],
                                    rows_ref[2, h : h + 1, there],
                                ),
                            )
                        pieces.append((scores[:, there] * jnp.exp(gap)).astype(jnp.bfloat16))
                    weights = jnp.concatenate(pieces, axis=1)
                    term = jnp.dot(weights, own, preferred_element_type=jnp.float32)
                    total = term if total is None else total + term
                out_ref[here, channels] = total


def close_kernel(sizes, info_ref, within_ref, readout_ref, cols_ref, states_ref, valve_ref, factor_ref, map_ref, send_ref, keep_ref):
    groups = readout_ref.shape[1] // STATE
    wide = within_ref.shape[1] // groups
    heads = cols_ref.shape[2]
    width = within_ref.shape[1] // heads
    lift_f = spread(jnp.exp(cols_ref[0]), width)
    lift_b = spread(jnp.exp(cols_ref[1]), width)
    blended = []
    for g in range(groups):
        at = slice(g * wide, (g + 1) * wide)
        readout = readout_ref[:, g * STATE : (g + 1) * STATE]
        carried_f = jnp.dot(readout, states_ref[0, :, at], preferred_element_type=jnp.float32)
        carried_b = jnp.dot(readout, states_ref[1, :, at], preferred_element_type=jnp.float32)
        mixed = within_ref[:, at] + carried_f * lift_f[:, at] + carried_b * lift_b[:, at]
        valve = valve_ref[:, at].astype(jnp.float32)
        gated = mixed * (valve / (1.0 + jnp.exp(-valve)))
        square = jnp.mean(gated * gated, axis=1, keepdims=True)
        scaled = gated * lax.rsqrt(square + EPSILON)
        blended.append((scaled * factor_ref[:, at]).astype(jnp.bfloat16))
    rows = jnp.concatenate(blended, axis=1)
    sp_count, count = sizes
    block = map_ref.shape[1] // count
    for p in range(count):
        columns = pl.ds(pl.multiple_of(info_ref[2 * sp_count + p] * block, block), block)
        term = jnp.dot(rows, map_ref[:, columns], preferred_element_type=jnp.float32).astype(jnp.bfloat16)
        target, at = (send_ref, p) if p < count // 2 else (keep_ref, p - count // 2)
        target[:, at * block : (at + 1) * block] = term


def up_kernel(sizes, plan, counts, *refs):
    n_pieces, n_arrays = counts
    sp_count, tp_count = sizes
    info_ref, gain_ref = refs[:2]
    pieces = refs[2 : 2 + n_pieces]
    arrays = refs[2 + n_pieces : 2 + n_pieces + n_arrays]
    outs = refs[2 + n_pieces + n_arrays : 4 + n_pieces + n_arrays]
    rows_scr, gain_scr = refs[4 + n_pieces + n_arrays :]
    length, full = pieces[0].shape[0], gain_ref.shape[1]
    chunk, block = full // sp_count, full // tp_count
    for p in range(tp_count):
        at = pl.multiple_of(info_ref[2 * sp_count + tp_count + p] * block, block)
        gain_scr[:, p * block : (p + 1) * block] = gain_ref[:, pl.ds(at, block)]

    band = 64

    def norm(r, carry):
        rows = pl.ds(pl.multiple_of(r * band, band), band)
        parts = [piece[rows, :].astype(jnp.float32) for piece in pieces]
        square = sum(jnp.sum(part * part, axis=1, keepdims=True) for part in parts) / full
        factor = lax.rsqrt(square + EPSILON)
        start = 0
        for part in parts:
            for first in range(0, part.shape[1], chunk):
                at = start + first
                rows_scr[at // chunk, rows, :] = (
                    part[:, first : first + chunk] * factor * gain_scr[:, at : at + chunk]
                ).astype(jnp.bfloat16)
            start += part.shape[1]
        return carry

    lax.fori_loop(0, length // band, norm, 0)
    columns = outs[0].shape[1]
    tile = 256 if columns % 256 == 0 else columns
    for which in range(2):
        for j in range(columns // tile):
            at = slice(j * tile, (j + 1) * tile)
            total = None
            for n, source in enumerate(plan[which]):
                term = jnp.dot(
                    rows_scr[info_ref[source] // chunk],
                    arrays[which * len(plan[0]) + n][:, at],
                    preferred_element_type=jnp.float32,
                )
                total = term if total is None else total + term
            outs[which][:, at] = total.astype(jnp.bfloat16)


def down_kernel(sizes, plan, blank, n_arrays, *refs):
    info_ref, hidden_ref = refs[:2]
    arrays = refs[2 : 2 + n_arrays]
    held = refs[2 + n_arrays : -2]
    outs = refs[-2:]
    half = outs[0].shape[1]
    for held_ref, out_ref in zip(held, outs):
        out_ref[...] = held_ref[...]

    def put(source, term):
        at = info_ref[sizes[0] + source]
        for side in range(2):

            @pl.when((at >= half) if side else (at < half))
            def _():
                columns = pl.ds(pl.multiple_of(at - side * half, term.shape[1]), term.shape[1])
                outs[side][:, columns] = term

    for source, parts in plan:
        term = down_term(hidden_ref, [(arrays[array], row) for array, row in parts])
        if term.shape[1] == 2 * half:
            outs[0][...] = term[:, :half]
            outs[1][...] = term[:, half:]
        else:
            put(source, term)
    if blank is not None:
        put(blank, jnp.zeros_like(term))


def down_term(hidden_ref, parts):
    term = None
    for array, row in parts:
        part = jnp.dot(
            hidden_ref[:, row : row + array.shape[0]], array[...], preferred_element_type=jnp.float32
        )
        term = part if term is None else term + part
    return term.astype(jnp.bfloat16)


def far_kernel(hidden_ref, top_ref, bottom_ref, out_ref):
    out_ref[...] = down_term(hidden_ref, [(top_ref, 0), (bottom_ref, top_ref.shape[0])])


def conv_rows(padded, kernel, length):
    summed = padded[0:length] * kernel[0]
    for offset in range(1, kernel.shape[0]):
        summed = summed + padded[offset : offset + length] * kernel[offset]
    return summed


def edges(last, first):
    count = lax.axis_size("sp")
    forward = [(i, i + 1) for i in range(count - 1)]
    backward = [(b, a) for a, b in forward]
    low = lax.ppermute(last, "sp", forward)
    high = lax.ppermute(first, "sp", backward)
    return low, high


def call(kernel, outs, *args, scalars=0, scratch=()):
    spaces = [pltpu.SMEM] * scalars + [pltpu.VMEM] * (len(args) - scalars)
    return pl.pallas_call(
        kernel,
        out_shape=[jax.ShapeDtypeStruct(shape, kind) for shape, kind in outs],
        in_specs=[pl.BlockSpec(memory_space=space) for space in spaces],
        scratch_shapes=list(scratch),
        compiler_params=pltpu.CompilerParams(vmem_limit_bytes=LIMIT * 1024 * 1024),
    )(*args)


def solution(mesh):
    cycle = ring_cycle(mesh)
    sp_count = mesh.shape["sp"]
    tp_count = mesh.shape["tp"]
    place = {s: i for i, s in enumerate(cycle)}
    right = [(cycle[i], cycle[(i + 1) % sp_count]) for i in range(sp_count)]
    left = [(b, a) for a, b in right]
    tp = Butterfly(tp_count)
    scatter_place = np.argsort(np.array(tp.scatter_mask))
    gather_place = np.argsort(np.array(tp.gather_mask))

    def table(chunk, own_cols):
        lines = []
        for s in range(sp_count):
            for t in range(tp_count):
                up, down = [], []
                for steps in range(sp_count):
                    block, rest = divmod(cycle[(place[s] - steps) % sp_count] * chunk, own_cols)
                    up.append(gather_place[block ^ t] * own_cols + rest)
                    down.append(scatter_place[block ^ t] * own_cols + rest)
                lines.append(up + down + [t ^ m for m in tp.scatter_mask] + [t ^ m for m in tp.gather_mask])
        return np.array(lines, np.int32)

    def send_on(array, pairs):
        return lax.ppermute(array, "sp", pairs)

    def ring(own, far_ways):
        out = []
        going, coming = own, own
        for step in range(1, (sp_count - 1) // 2 + 1):
            going = send_on(going, right)
            coming = send_on(coming, left)
            out += [(step, going, 0), (-step, coming, 0)]
        if sp_count % 2 == 0:
            far = sp_count // 2
            half = own.shape[0] // 2
            if far_ways == "f":
                out.append((far, send_on(going, right), 0))
            elif far_ways == "b":
                out.append((far, send_on(coming, left), 0))
            else:
                out.append((far, send_on(going[:half], right), 0))
                out.append((far, send_on(coming[half:], left), half))
        return out

    def shards(
        skip_trunk_vector,
        valve_preactivation,
        projected_heads_payload,
        cluster_ingests,
        cluster_observers,
        pre_softplus_increments,
        attenuation_ln_rate,
        additional_attenuation,
        payload_conv_weights,
        ingest_conv_weights,
        observer_conv_weights,
        valved_cluster_factor,
        closing_map_matrix,
        dense_standardize_factor,
        dense_valve_map,
        dense_payload_map,
        valve_series_smoother,
        payload_series_smoother,
        dense_contract_map,
    ):
        length = skip_trunk_vector.shape[0]
        heads = pre_softplus_increments.shape[2]
        channels = projected_heads_payload.shape[1]
        in_cols = cluster_ingests.shape[1]
        own_cols = skip_trunk_vector.shape[1]
        me = lax.axis_index("tp")

        margin = payload_conv_weights.shape[0] // 2
        streams = (projected_heads_payload, cluster_ingests, cluster_observers)
        low, high = edges(
            jnp.concatenate([a[length - margin :] for a in streams], axis=1),
            jnp.concatenate([a[:margin] for a in streams], axis=1),
        )

        full = own_cols * tp_count
        hidden_cols = dense_valve_map.shape[1]
        chunk = dense_valve_map.shape[0]
        up_rings = [[(0, own, 0)] + ring(own, way) for own, way in ((dense_valve_map, "f"), (dense_payload_map, "b"))]
        down_ring = [(0, dense_contract_map, 0)] + ring(dense_contract_map, "fb")
        info = jnp.asarray(table(chunk, own_cols))[lax.axis_index("sp") * tp_count + me]

        rows, cols, scale, last = call(
            decay_kernel,
            [
                ((3, heads, length), jnp.float32),
                ((2, length, heads), jnp.float32),
                ((2, length, channels), jnp.float32),
                ((2, 8, channels), jnp.float32),
            ],
            jnp.transpose(pre_softplus_increments, (0, 2, 1)),
            jnp.transpose(additional_attenuation, (0, 2, 1)),
            attenuation_ln_rate.T,
        )

        def mixed(array, low, high, kernel):
            padded = jnp.concatenate([low, array, high], axis=0).astype(jnp.float32)
            return jax.nn.silu(conv_rows(padded, kernel, length)).astype(jnp.bfloat16)

        ends = (channels, channels + in_cols)
        lows, highs = jnp.split(low, ends, axis=1), jnp.split(high, ends, axis=1)
        values = mixed(projected_heads_payload, lows[0], highs[0], payload_conv_weights)
        inputs = mixed(cluster_ingests, lows[1], highs[1], ingest_conv_weights)
        readout = mixed(cluster_observers, lows[2], highs[2], observer_conv_weights)
        wide_state = ((2, STATE + 8, channels), jnp.float32)
        sent = ((STATE + TAIL, channels), jnp.bfloat16)
        window, send_f, send_b = call(
            state_kernel, [wide_state, sent, sent], values, inputs, scale, last
        )
        (within,) = call(
            within_kernel, [((length, channels), jnp.float32)], values, inputs, readout, rows, cols
        )

        before, offset = (), 1
        while offset < sp_count:
            forward = [(i, i + offset) for i in range(sp_count - offset)]
            got_f = lax.ppermute(send_f, "sp", forward)
            got_b = lax.ppermute(send_b, "sp", [(b, a) for a, b in forward])
            final = 2 * offset >= sp_count
            outs = [((2, STATE, channels), jnp.bfloat16)]
            if not final:
                outs = [wide_state, wide_state, sent, sent]
            result = call(
                functools.partial(link_kernel, offset == 1, final),
                outs,
                got_f,
                got_b,
                *before,
                *(() if final else (window,)),
            )
            if final:
                states = result[0]
            else:
                before, (window, send_f, send_b) = (result[0],), result[1:]
            offset *= 2

        half_full = full // 2
        send, keep = call(
            functools.partial(close_kernel, (sp_count, tp_count)),
            [((length, half_full), jnp.bfloat16)] * 2,
            info,
            within,
            readout,
            cols,
            states,
            valve_preactivation,
            valved_cluster_factor[None, :],
            closing_map_matrix,
            scalars=1,
        )
        projected = tp.reduce_scatter(send, keep)
        middle = (skip_trunk_vector.astype(jnp.float32) + projected).astype(jnp.bfloat16)
        pieces = tp.gather(middle)

        arrays = [array for entries in up_rings for _, array, _ in entries]
        plan = [[steps % sp_count for steps, _, _ in entries] for entries in up_rings]
        gate_rows, value_rows = call(
            functools.partial(up_kernel, (sp_count, tp_count), plan, (len(pieces), len(arrays))),
            [((length, hidden_cols), jnp.bfloat16)] * 2,
            info,
            dense_standardize_factor[None, :],
            *pieces,
            *arrays,
            scalars=1,
            scratch=[pltpu.VMEM((sp_count, length, chunk), jnp.bfloat16), pltpu.VMEM((1, full), jnp.float32)],
        )
        margin = valve_series_smoother.shape[0] // 2
        low, high = edges(
            jnp.concatenate([gate_rows[length - margin :], value_rows[length - margin :]], axis=1),
            jnp.concatenate([gate_rows[:margin], value_rows[:margin]], axis=1),
        )

        def smooth(array, low, high, kernel):
            return conv_rows(jnp.concatenate([low, array, high], axis=0).astype(jnp.float32), kernel, length)

        gate = smooth(gate_rows, low[:, :hidden_cols], high[:, :hidden_cols], valve_series_smoother)
        value = smooth(value_rows, low[:, hidden_cols:], high[:, hidden_cols:], payload_series_smoother)
        hidden = (jax.nn.silu(gate) * value).astype(jnp.bfloat16)

        def down(plan, blank, arrays, held=()):
            return call(
                functools.partial(down_kernel, (sp_count, tp_count), plan, blank, len(arrays)),
                [((length, half_full), jnp.bfloat16)] * 2,
                info,
                hidden,
                *arrays,
                *held,
                scalars=1,
            )

        if chunk % 128:
            whole = jnp.zeros((hidden_cols, full), jnp.bfloat16)
            for steps, array, first in down_ring:
                whole = lax.dynamic_update_slice(whole, array, (first, info[sp_count + steps % sp_count]))
            send, keep = down([(0, [(0, 0)])], None, [whole])
            down_sum = tp.reduce_scatter(send, keep)
            return (middle.astype(jnp.float32) + down_sum).astype(jnp.bfloat16)

        far = sp_count // 2
        near_chunks = [(steps % sp_count, array) for steps, array, _ in down_ring if abs(steps) < far]
        early, late = near_chunks[:-2], near_chunks[-2:]
        held = down([(slot, [(n, 0)]) for n, (slot, _) in enumerate(early)], None, [a for _, a in early])
        send, keep = down([(slot, [(n, 0)]) for n, (slot, _) in enumerate(late)], far, [a for _, a in late], held)
        down_sum = tp.reduce_scatter(send, keep)
        (part,) = call(
            far_kernel, [((length, chunk), jnp.bfloat16)], hidden, *(a for _, a, _ in down_ring[-2:])
        )
        for bit in range(tp.bits):
            pairs = []
            for s in range(sp_count):
                owner = cycle[(place[s] - far) % sp_count] * chunk // own_cols
                for t in range(tp_count):
                    apart = t ^ owner
                    if apart >> bit & 1 and apart % (1 << bit) == 0:
                        pairs.append((s * tp_count + t, s * tp_count + (t ^ (1 << bit))))
            received = lax.ppermute(part.astype(jnp.bfloat16), ("sp", "tp"), pairs)
            part = part.astype(jnp.float32) + received.astype(jnp.float32)
        at = info[sp_count + far] - (tp_count - 1) * own_cols
        spots = range(0, own_cols, chunk)
        placed = jnp.concatenate([jnp.where(at == spot, part, 0.0) for spot in spots], axis=1)
        return (middle.astype(jnp.float32) + down_sum + placed).astype(jnp.bfloat16)

    return jax.shard_map(
        shards,
        mesh=mesh,
        in_specs=(
            P("sp", "tp"),
            P("sp", "tp"),
            P("sp", "tp"),
            P("sp", "tp"),
            P("sp", "tp"),
            P(None, "sp", "tp"),
            P(None, "tp"),
            P(None, "sp", "tp"),
            P(None, "tp"),
            P(None, "tp"),
            P(None, "tp"),
            P("tp"),
            P("tp", None),
            P(),
            P("sp", "tp"),
            P("sp", "tp"),
            P(None, "tp"),
            P(None, "tp"),
            P("tp", "sp"),
        ),
        out_specs=P("sp", "tp"),
        check_vma=False,
    )
```

```python
import functools

import jax
import jax.numpy as jnp
import numpy as np
from jax import lax
from jax.experimental import pallas as pl
from jax.experimental.pallas import tpu as pltpu
from jax.sharding import PartitionSpec as P


STATE = 128
EPSILON = 1e-06
TAIL = 16
LIMIT = 16


def ring_cycle(mesh):
    line = mesh.devices[:, 0].ravel()
    count = len(line)
    if not all(hasattr(d, "coords") for d in line):
        return list(range(count))
    spots = {(d.coords[2], d.coords[1]): i for i, d in enumerate(line)}
    deep = sorted({z for z, _ in spots})
    wide = sorted({y for _, y in spots})
    if len(spots) != count or len(deep) % 2 or len(wide) < 2:
        return list(range(count))
    path = []
    for at, z in enumerate(deep):
        row = wide[1:] if at % 2 == 0 else wide[:0:-1]
        path += [(z, y) for y in row]
    path += [(z, wide[0]) for z in reversed(deep)]
    return [spots[spot] for spot in path]


def bit_reverse(value, bits):
    return int(format(value, f"0{bits}b")[::-1], 2) if bits else 0


class Butterfly:
    def __init__(self, count):
        self.count = count
        self.bits = count.bit_length() - 1
        self.scatter_mask = [bit_reverse(count - 1 - p, self.bits) for p in range(count)]
        self.gather_mask = [bit_reverse(p, self.bits) for p in range(count)]

    def swap(self, array, bit):
        return lax.ppermute(array, "tp", [(i, i ^ (1 << bit)) for i in range(self.count)])

    def reduce_scatter(self, send, keep):
        for bit in range(self.bits):
            received = self.swap(send.astype(jnp.bfloat16), bit)
            held = keep.astype(jnp.float32) + received.astype(jnp.float32)
            half = held.shape[1] // 2
            send, keep = held[:, :half], held[:, half:]
        return held

    def gather(self, own):
        pieces = [own]
        for bit in reversed(range(self.bits)):
            held = pieces[0] if len(pieces) == 1 else jnp.concatenate(pieces, axis=1)
            pieces.append(self.swap(held, bit))
        return pieces


def softplus(v):
    return jnp.maximum(v, 0.0) + jnp.log1p(jnp.exp(-jnp.abs(v)))


def three(v, axis):
    high = v.astype(jnp.bfloat16)
    rest = v - high.astype(jnp.float32)
    mid = rest.astype(jnp.bfloat16)
    low = (rest - mid.astype(jnp.float32)).astype(jnp.bfloat16)
    return jnp.concatenate([high, mid, low], axis=axis)


def spread(v, width):
    heads = v.shape[1]
    high = v.astype(jnp.bfloat16)
    low = (v - high.astype(jnp.float32)).astype(jnp.bfloat16)
    row = lax.broadcasted_iota(jnp.int32, (2 * heads, heads * width), 0)
    column = lax.broadcasted_iota(jnp.int32, (2 * heads, heads * width), 1) // width
    pick = ((row == column) | (row - heads == column)).astype(jnp.float32).astype(jnp.bfloat16)
    return jnp.dot(
        jnp.concatenate([high, low], axis=1), pick, preferred_element_type=jnp.float32
    )


def decay_kernel(pre_ref, add_ref, rate_ref, rows_ref, cols_ref, scale_ref, last_ref):
    _, heads, length = pre_ref.shape
    width = scale_ref.shape[2] // heads
    at0 = lax.broadcasted_iota(jnp.int32, (length, length), 0)
    at1 = lax.broadcasted_iota(jnp.int32, (length, length), 1)
    steps, runs = [], []
    for way in range(2):
        reach = (at0 <= at1) if way == 0 else (at0 >= at1)
        reach = reach.astype(jnp.float32).astype(jnp.bfloat16)
        step = softplus(pre_ref[way])
        log = add_ref[way] - step * jnp.exp(rate_ref[:, way : way + 1])
        sums = jnp.dot(three(log, 0), reach, preferred_element_type=jnp.float32)
        run = sums[:heads] + sums[heads : 2 * heads] + sums[2 * heads :]
        rows_ref[way] = jnp.log(step) - run
        steps.append(step)
        runs.append(run)
    rows_ref[2] = jnp.log(steps[0] + steps[1])
    rest = jnp.zeros((128 - 4 * heads, length), jnp.float32)
    turned = jnp.concatenate([*runs, *steps, rest], axis=0).T
    for way in range(2):
        down = turned[:, way * heads : (way + 1) * heads]
        step = turned[:, (2 + way) * heads : (3 + way) * heads]
        end = down[length - 1 : length] if way == 0 else down[0:1]
        cols_ref[way] = down
        scale_ref[way] = spread(jnp.exp(end - down) * step, width)
        last_ref[way] = spread(jnp.broadcast_to(jnp.exp(end), (8, heads)), width)


def message(state, decay):
    high = decay.astype(jnp.bfloat16).astype(jnp.float32)
    low = decay - high
    row = lax.broadcasted_iota(jnp.int32, (TAIL, state.shape[1]), 0)
    tail = jnp.where(row == 0, high, jnp.where(row == 1, low, 0.0))
    return jnp.concatenate([state, tail], axis=0).astype(jnp.bfloat16)


def state_kernel(values_ref, inputs_ref, scale_ref, last_ref, window_ref, send_f_ref, send_b_ref):
    groups = inputs_ref.shape[1] // STATE
    wide = values_ref.shape[1] // groups
    values = values_ref[...].astype(jnp.float32)
    for way, send_ref in enumerate((send_f_ref, send_b_ref)):
        scaled = (values * scale_ref[way]).astype(jnp.bfloat16)
        state = jnp.concatenate(
            [
                lax.dot_general(
                    inputs_ref[:, g * STATE : (g + 1) * STATE],
                    scaled[:, g * wide : (g + 1) * wide],
                    (((0,), (0,)), ((), ())),
                    preferred_element_type=jnp.float32,
                )
                for g in range(groups)
            ],
            axis=1,
        )
        window_ref[way, :STATE] = state
        window_ref[way, STATE:] = last_ref[way]
        send_ref[...] = message(state, last_ref[way, 0:1])


def link_kernel(first, final, *refs):
    got_refs, refs = refs[:2], list(refs[2:])
    before_ref = None if first else refs.pop(0)
    window_ref = None if final else refs.pop(0)
    for way in range(2):
        got = got_refs[way][:STATE].astype(jnp.float32)
        got_decay = got_refs[way][STATE : STATE + 1].astype(jnp.float32) + got_refs[way][
            STATE + 1 : STATE + 2
        ].astype(jnp.float32)
        before, before_decay = got, got_decay
        if not first:
            held_decay = before_ref[way, STATE : STATE + 1]
            before = got * held_decay + before_ref[way, :STATE]
            before_decay = got_decay * held_decay
        if final:
            refs[0][way] = before.astype(jnp.bfloat16)
            continue
        decay = window_ref[way, STATE : STATE + 1]
        state = got * decay + window_ref[way, :STATE]
        decay = decay * got_decay
        for ref, value, factor in ((refs[0], before, before_decay), (refs[1], state, decay)):
            ref[way, :STATE] = value
            ref[way, STATE:] = jnp.broadcast_to(factor, (8, factor.shape[1]))
        refs[2 + way][...] = message(state, decay)


def within_kernel(values_ref, inputs_ref, readout_ref, rows_ref, cols_ref, out_ref):
    heads = rows_ref.shape[1]
    length = values_ref.shape[0]
    width = values_ref.shape[1] // heads
    tile = min(256, length)
    groups = inputs_ref.shape[1] // STATE
    per_group = heads // groups
    pack = max(1, 128 // width)
    lane = lax.broadcasted_iota(jnp.int32, (length, pack * width), 1) // width
    at0 = lax.broadcasted_iota(jnp.int32, (tile, tile), 0)
    at1 = lax.broadcasted_iota(jnp.int32, (tile, tile), 1)
    for g in range(groups):
        for i in range(length // tile):
            here = slice(i * tile, (i + 1) * tile)
            scores = lax.dot_general(
                readout_ref[here, g * STATE : (g + 1) * STATE],
                inputs_ref[:, g * STATE : (g + 1) * STATE],
                (((1,), (1,)), ((), ())),
                preferred_element_type=jnp.float32,
            )
            for first in range(0, per_group, pack):
                total = None
                channels = slice((g * per_group + first) * width, (g * per_group + first + pack) * width)
                packed = values_ref[:, channels]
                for sub in range(pack):
                    h = g * per_group + first + sub
                    own = jnp.where(lane == sub, packed, jnp.zeros_like(packed))
                    down_f = cols_ref[0, here, h : h + 1]
                    down_b = cols_ref[1, here, h : h + 1]
                    pieces = []
                    for j in range(length // tile):
                        there = slice(j * tile, (j + 1) * tile)
                        if i > j:
                            gap = down_f + rows_ref[0, h : h + 1, there]
                        elif i < j:
                            gap = down_b + rows_ref[1, h : h + 1, there]
                        else:
                            gap = jnp.where(
                                at0 > at1,
                                down_f + rows_ref[0, h : h + 1, there],
                                jnp.where(
                                    at0 < at1,
                                    down_b + rows_ref[1, h : h + 1, there],
                                    rows_ref[2, h : h + 1, there],
                                ),
                            )
                        pieces.append((scores[:, there] * jnp.exp(gap)).astype(jnp.bfloat16))
                    weights = jnp.concatenate(pieces, axis=1)
                    term = jnp.dot(weights, own, preferred_element_type=jnp.float32)
                    total = term if total is None else total + term
                out_ref[here, channels] = total


def close_kernel(sizes, info_ref, within_ref, readout_ref, cols_ref, states_ref, valve_ref, factor_ref, map_ref, send_ref, keep_ref):
    groups = readout_ref.shape[1] // STATE
    wide = within_ref.shape[1] // groups
    heads = cols_ref.shape[2]
    width = within_ref.shape[1] // heads
    lift_f = spread(jnp.exp(cols_ref[0]), width)
    lift_b = spread(jnp.exp(cols_ref[1]), width)
    blended = []
    for g in range(groups):
        at = slice(g * wide, (g + 1) * wide)
        readout = readout_ref[:, g * STATE : (g + 1) * STATE]
        carried_f = jnp.dot(readout, states_ref[0, :, at], preferred_element_type=jnp.float32)
        carried_b = jnp.dot(readout, states_ref[1, :, at], preferred_element_type=jnp.float32)
        mixed = within_ref[:, at] + carried_f * lift_f[:, at] + carried_b * lift_b[:, at]
        valve = valve_ref[:, at].astype(jnp.float32)
        gated = mixed * (valve / (1.0 + jnp.exp(-valve)))
        square = jnp.mean(gated * gated, axis=1, keepdims=True)
        scaled = gated * lax.rsqrt(square + EPSILON)
        blended.append((scaled * factor_ref[:, at]).astype(jnp.bfloat16))
    rows = jnp.concatenate(blended, axis=1)
    sp_count, count = sizes
    block = map_ref.shape[1] // count
    for p in range(count):
        columns = pl.ds(pl.multiple_of(info_ref[2 * sp_count + p] * block, block), block)
        term = jnp.dot(rows, map_ref[:, columns], preferred_element_type=jnp.float32).astype(jnp.bfloat16)
        target, at = (send_ref, p) if p < count // 2 else (keep_ref, p - count // 2)
        target[:, at * block : (at + 1) * block] = term


def up_kernel(sizes, plan, counts, last, *refs):
    n_pieces, n_arrays = counts
    sp_count, tp_count = sizes
    info_ref, gain_ref = refs[:2]
    pieces = refs[2 : 2 + n_pieces]
    arrays = refs[2 + n_pieces : 2 + n_pieces + n_arrays]
    outs = refs[2 + n_pieces + n_arrays : 4 + n_pieces + n_arrays]
    last_ref, rows_scr, gain_scr = refs[4 + n_pieces + n_arrays :]
    length, full = pieces[0].shape[0], gain_ref.shape[1]
    chunk, block = full // sp_count, full // tp_count
    for p in range(tp_count):
        at = pl.multiple_of(info_ref[2 * sp_count + tp_count + p] * block, block)
        gain_scr[:, p * block : (p + 1) * block] = gain_ref[:, pl.ds(at, block)]

    band = 64

    def norm(r, carry):
        rows = pl.ds(pl.multiple_of(r * band, band), band)
        parts = [piece[rows, :].astype(jnp.float32) for piece in pieces]
        square = sum(jnp.sum(part * part, axis=1, keepdims=True) for part in parts) / full
        factor = lax.rsqrt(square + EPSILON)
        start = 0
        for part in parts:
            for first in range(0, part.shape[1], chunk):
                at = start + first
                rows_scr[at // chunk, rows, :] = (
                    part[:, first : first + chunk] * factor * gain_scr[:, at : at + chunk]
                ).astype(jnp.bfloat16)
            start += part.shape[1]
        return carry

    lax.fori_loop(0, length // band, norm, 0)
    last_ref[...] = rows_scr[info_ref[last] // chunk]
    columns = outs[0].shape[1]
    tile = 256 if columns % 256 == 0 else columns
    for which in range(2):
        for j in range(columns // tile):
            at = slice(j * tile, (j + 1) * tile)
            total = None
            for n, source in enumerate(plan[which]):
                term = jnp.dot(
                    rows_scr[info_ref[source] // chunk],
                    arrays[which * len(plan[0]) + n][:, at],
                    preferred_element_type=jnp.float32,
                )
                total = term if total is None else total + term
            outs[which][:, at] = total


def up_last_kernel(gate_ref, value_ref, rows_ref, gate_map_ref, value_map_ref, gate_out, value_out):
    columns = gate_ref.shape[1]
    tile = 256 if columns % 256 == 0 else columns
    for held, map_ref, out in ((gate_ref, gate_map_ref, gate_out), (value_ref, value_map_ref, value_out)):
        for j in range(columns // tile):
            at = slice(j * tile, (j + 1) * tile)
            term = jnp.dot(rows_ref[...], map_ref[:, at], preferred_element_type=jnp.float32)
            out[:, at] = (held[:, at] + term).astype(jnp.bfloat16)


def down_kernel(sizes, plan, blank, n_arrays, *refs):
    info_ref, hidden_ref = refs[:2]
    arrays = refs[2 : 2 + n_arrays]
    held = refs[2 + n_arrays : -2]
    outs = refs[-2:]
    half = outs[0].shape[1]
    for held_ref, out_ref in zip(held, outs):
        out_ref[...] = held_ref[...]

    def put(source, term):
        at = info_ref[sizes[0] + source]
        for side in range(2):

            @pl.when((at >= half) if side else (at < half))
            def _():
                columns = pl.ds(pl.multiple_of(at - side * half, term.shape[1]), term.shape[1])
                outs[side][:, columns] = term

    for source, parts in plan:
        term = down_term(hidden_ref, [(arrays[array], row) for array, row in parts])
        if term.shape[1] == 2 * half:
            outs[0][...] = term[:, :half]
            outs[1][...] = term[:, half:]
        else:
            put(source, term)
    if blank is not None:
        put(blank, jnp.zeros_like(term))


def down_term(hidden_ref, parts):
    term = None
    for array, row in parts:
        part = jnp.dot(
            hidden_ref[:, row : row + array.shape[0]], array[...], preferred_element_type=jnp.float32
        )
        term = part if term is None else term + part
    return term.astype(jnp.bfloat16)


def far_kernel(hidden_ref, top_ref, bottom_ref, out_ref):
    out_ref[...] = down_term(hidden_ref, [(top_ref, 0), (bottom_ref, top_ref.shape[0])])


def conv_rows(padded, kernel, length):
    summed = padded[0:length] * kernel[0]
    for offset in range(1, kernel.shape[0]):
        summed = summed + padded[offset : offset + length] * kernel[offset]
    return summed


def edges(last, first):
    count = lax.axis_size("sp")
    forward = [(i, i + 1) for i in range(count - 1)]
    backward = [(b, a) for a, b in forward]
    low = lax.ppermute(last, "sp", forward)
    high = lax.ppermute(first, "sp", backward)
    return low, high


def call(kernel, outs, *args, scalars=0, scratch=()):
    spaces = [pltpu.SMEM] * scalars + [pltpu.VMEM] * (len(args) - scalars)
    return pl.pallas_call(
        kernel,
        out_shape=[jax.ShapeDtypeStruct(shape, kind) for shape, kind in outs],
        in_specs=[pl.BlockSpec(memory_space=space) for space in spaces],
        scratch_shapes=list(scratch),
        compiler_params=pltpu.CompilerParams(vmem_limit_bytes=LIMIT * 1024 * 1024),
    )(*args)


def solution(mesh):
    cycle = ring_cycle(mesh)
    sp_count = mesh.shape["sp"]
    tp_count = mesh.shape["tp"]
    place = {s: i for i, s in enumerate(cycle)}
    right = [(cycle[i], cycle[(i + 1) % sp_count]) for i in range(sp_count)]
    left = [(b, a) for a, b in right]
    tp = Butterfly(tp_count)
    scatter_place = np.argsort(np.array(tp.scatter_mask))
    gather_place = np.argsort(np.array(tp.gather_mask))

    def table(chunk, own_cols):
        lines = []
        for s in range(sp_count):
            for t in range(tp_count):
                up, down = [], []
                for steps in range(sp_count):
                    block, rest = divmod(cycle[(place[s] - steps) % sp_count] * chunk, own_cols)
                    up.append(gather_place[block ^ t] * own_cols + rest)
                    down.append(scatter_place[block ^ t] * own_cols + rest)
                lines.append(up + down + [t ^ m for m in tp.scatter_mask] + [t ^ m for m in tp.gather_mask])
        return np.array(lines, np.int32)

    def send_on(array, pairs):
        return lax.ppermute(array, "sp", pairs)

    def ring(own, far_ways):
        out = []
        going, coming = own, own
        for step in range(1, (sp_count - 1) // 2 + 1):
            going = send_on(going, right)
            coming = send_on(coming, left)
            out += [(step, going, 0), (-step, coming, 0)]
        if sp_count % 2 == 0:
            far = sp_count // 2
            half = own.shape[0] // 2
            if far_ways == "f":
                out.append((far, send_on(going, right), 0))
            elif far_ways == "b":
                out.append((far, send_on(coming, left), 0))
            else:
                out.append((far, send_on(going[:half], right), 0))
                out.append((far, send_on(coming[half:], left), half))
        return out

    def shards(
        skip_trunk_vector,
        valve_preactivation,
        projected_heads_payload,
        cluster_ingests,
        cluster_observers,
        pre_softplus_increments,
        attenuation_ln_rate,
        additional_attenuation,
        payload_conv_weights,
        ingest_conv_weights,
        observer_conv_weights,
        valved_cluster_factor,
        closing_map_matrix,
        dense_standardize_factor,
        dense_valve_map,
        dense_payload_map,
        valve_series_smoother,
        payload_series_smoother,
        dense_contract_map,
    ):
        length = skip_trunk_vector.shape[0]
        heads = pre_softplus_increments.shape[2]
        channels = projected_heads_payload.shape[1]
        in_cols = cluster_ingests.shape[1]
        own_cols = skip_trunk_vector.shape[1]
        me = lax.axis_index("tp")

        margin = payload_conv_weights.shape[0] // 2
        streams = (projected_heads_payload, cluster_ingests, cluster_observers)
        low, high = edges(
            jnp.concatenate([a[length - margin :] for a in streams], axis=1),
            jnp.concatenate([a[:margin] for a in streams], axis=1),
        )

        full = own_cols * tp_count
        hidden_cols = dense_valve_map.shape[1]
        chunk = dense_valve_map.shape[0]
        up_rings = [[(0, own, 0)] + ring(own, way) for own, way in ((dense_valve_map, "f"), (dense_payload_map, "b"))]
        half_row = hidden_cols // 2
        down_rings = [
            [(0, own, 0)] + ring(own, way)
            for own, way in ((dense_contract_map[:half_row], "f"), (dense_contract_map[half_row:], "b"))
        ]
        info = jnp.asarray(table(chunk, own_cols))[lax.axis_index("sp") * tp_count + me]

        rows, cols, scale, last = call(
            decay_kernel,
            [
                ((3, heads, length), jnp.float32),
                ((2, length, heads), jnp.float32),
                ((2, length, channels), jnp.float32),
                ((2, 8, channels), jnp.float32),
            ],
            jnp.transpose(pre_softplus_increments, (0, 2, 1)),
            jnp.transpose(additional_attenuation, (0, 2, 1)),
            attenuation_ln_rate.T,
        )

        def mixed(array, low, high, kernel):
            padded = jnp.concatenate([low, array, high], axis=0).astype(jnp.float32)
            return jax.nn.silu(conv_rows(padded, kernel, length)).astype(jnp.bfloat16)

        ends = (channels, channels + in_cols)
        lows, highs = jnp.split(low, ends, axis=1), jnp.split(high, ends, axis=1)
        values = mixed(projected_heads_payload, lows[0], highs[0], payload_conv_weights)
        inputs = mixed(cluster_ingests, lows[1], highs[1], ingest_conv_weights)
        readout = mixed(cluster_observers, lows[2], highs[2], observer_conv_weights)
        wide_state = ((2, STATE + 8, channels), jnp.float32)
        sent = ((STATE + TAIL, channels), jnp.bfloat16)
        window, send_f, send_b = call(
            state_kernel, [wide_state, sent, sent], values, inputs, scale, last
        )
        (within,) = call(
            within_kernel, [((length, channels), jnp.float32)], values, inputs, readout, rows, cols
        )

        before, offset = (), 1
        while offset < sp_count:
            forward = [(i, i + offset) for i in range(sp_count - offset)]
            got_f = lax.ppermute(send_f, "sp", forward)
            got_b = lax.ppermute(send_b, "sp", [(b, a) for a, b in forward])
            final = 2 * offset >= sp_count
            outs = [((2, STATE, channels), jnp.bfloat16)]
            if not final:
                outs = [wide_state, wide_state, sent, sent]
            result = call(
                functools.partial(link_kernel, offset == 1, final),
                outs,
                got_f,
                got_b,
                *before,
                *(() if final else (window,)),
            )
            if final:
                states = result[0]
            else:
                before, (window, send_f, send_b) = (result[0],), result[1:]
            offset *= 2

        half_full = full // 2
        send, keep = call(
            functools.partial(close_kernel, (sp_count, tp_count)),
            [((length, half_full), jnp.bfloat16)] * 2,
            info,
            within,
            readout,
            cols,
            states,
            valve_preactivation,
            valved_cluster_factor[None, :],
            closing_map_matrix,
            scalars=1,
        )
        projected = tp.reduce_scatter(send, keep)
        middle = (skip_trunk_vector.astype(jnp.float32) + projected).astype(jnp.bfloat16)
        pieces = tp.gather(middle)

        arrays = [array for entries in up_rings for _, array, _ in entries[:-1]]
        plan = [[steps % sp_count for steps, _, _ in entries[:-1]] for entries in up_rings]
        last = up_rings[0][-1][0] % sp_count
        gate_sum, value_sum, last_rows = call(
            functools.partial(up_kernel, (sp_count, tp_count), plan, (len(pieces), len(arrays)), last),
            [((length, hidden_cols), jnp.float32)] * 2 + [((length, chunk), jnp.bfloat16)],
            info,
            dense_standardize_factor[None, :],
            *pieces,
            *arrays,
            scalars=1,
            scratch=[pltpu.VMEM((sp_count, length, chunk), jnp.bfloat16), pltpu.VMEM((1, full), jnp.float32)],
        )
        gate_rows, value_rows = call(
            up_last_kernel,
            [((length, hidden_cols), jnp.bfloat16)] * 2,
            gate_sum,
            value_sum,
            last_rows,
            *(entries[-1][1] for entries in up_rings),
        )
        margin = valve_series_smoother.shape[0] // 2
        low, high = edges(
            jnp.concatenate([gate_rows[length - margin :], value_rows[length - margin :]], axis=1),
            jnp.concatenate([gate_rows[:margin], value_rows[:margin]], axis=1),
        )

        def smooth(array, low, high, kernel):
            return conv_rows(jnp.concatenate([low, array, high], axis=0).astype(jnp.float32), kernel, length)

        gate = smooth(gate_rows, low[:, :hidden_cols], high[:, :hidden_cols], valve_series_smoother)
        value = smooth(value_rows, low[:, hidden_cols:], high[:, hidden_cols:], payload_series_smoother)
        hidden = (jax.nn.silu(gate) * value).astype(jnp.bfloat16)

        def down(plan, blank, arrays, held=()):
            return call(
                functools.partial(down_kernel, (sp_count, tp_count), plan, blank, len(arrays)),
                [((length, half_full), jnp.bfloat16)] * 2,
                info,
                hidden,
                *arrays,
                *held,
                scalars=1,
            )

        if chunk % 128:
            whole = jnp.zeros((hidden_cols, full), jnp.bfloat16)
            for part, entries in enumerate(down_rings):
                for steps, array, _ in entries:
                    corner = (part * half_row, info[sp_count + steps % sp_count])
                    whole = lax.dynamic_update_slice(whole, array, corner)
            send, keep = down([(0, [(0, 0)])], None, [whole])
            down_sum = tp.reduce_scatter(send, keep)
            return (middle.astype(jnp.float32) + down_sum).astype(jnp.bfloat16)

        far = sp_count // 2
        pairs = [
            (steps % sp_count, (top, bottom)) for (steps, top, _), (_, bottom, _) in zip(*down_rings) if abs(steps) < far
        ]

        def part_of(chunks, blank, held=()):
            plan = [(slot, [(2 * n, 0), (2 * n + 1, half_row)]) for n, (slot, _) in enumerate(chunks)]
            return down(plan, blank, [array for _, both_parts in chunks for array in both_parts], held)

        early = part_of(pairs[:-2], None)
        send, keep = part_of(pairs[-2:], far, early)
        down_sum = tp.reduce_scatter(send, keep)
        (part,) = call(
            far_kernel, [((length, chunk), jnp.bfloat16)], hidden, *(entries[-1][1] for entries in down_rings)
        )
        for bit in range(tp.bits):
            pairs = []
            for s in range(sp_count):
                owner = cycle[(place[s] - far) % sp_count] * chunk // own_cols
                for t in range(tp_count):
                    apart = t ^ owner
                    if apart >> bit & 1 and apart % (1 << bit) == 0:
                        pairs.append((s * tp_count + t, s * tp_count + (t ^ (1 << bit))))
            received = lax.ppermute(part.astype(jnp.bfloat16), ("sp", "tp"), pairs)
            part = part.astype(jnp.float32) + received.astype(jnp.float32)
        at = info[sp_count + far] - (tp_count - 1) * own_cols
        spots = range(0, own_cols, chunk)
        placed = jnp.concatenate([jnp.where(at == spot, part, 0.0) for spot in spots], axis=1)
        return (middle.astype(jnp.float32) + down_sum + placed).astype(jnp.bfloat16)

    return jax.shard_map(
        shards,
        mesh=mesh,
        in_specs=(
            P("sp", "tp"),
            P("sp", "tp"),
            P("sp", "tp"),
            P("sp", "tp"),
            P("sp", "tp"),
            P(None, "sp", "tp"),
            P(None, "tp"),
            P(None, "sp", "tp"),
            P(None, "tp"),
            P(None, "tp"),
            P(None, "tp"),
            P("tp"),
            P("tp", None),
            P(),
            P("sp", "tp"),
            P("sp", "tp"),
            P(None, "tp"),
            P(None, "tp"),
            P("tp", "sp"),
        ),
        out_specs=P("sp", "tp"),
        check_vma=False,
    )
```

```python
import functools

import jax
import jax.numpy as jnp
import numpy as np
from jax import lax
from jax.experimental import pallas as pl
from jax.experimental.pallas import tpu as pltpu
from jax.sharding import PartitionSpec as P


STATE = 128
EPSILON = 1e-06
TAIL = 16
LIMIT = 16


def ring_cycle(mesh):
    line = mesh.devices[:, 0].ravel()
    count = len(line)
    if not all(hasattr(d, "coords") for d in line):
        return list(range(count))
    spots = {(d.coords[2], d.coords[1]): i for i, d in enumerate(line)}
    deep = sorted({z for z, _ in spots})
    wide = sorted({y for _, y in spots})
    if len(spots) != count or len(deep) % 2 or len(wide) < 2:
        return list(range(count))
    path = []
    for at, z in enumerate(deep):
        row = wide[1:] if at % 2 == 0 else wide[:0:-1]
        path += [(z, y) for y in row]
    path += [(z, wide[0]) for z in reversed(deep)]
    return [spots[spot] for spot in path]


def bit_reverse(value, bits):
    return int(format(value, f"0{bits}b")[::-1], 2) if bits else 0


class Butterfly:
    def __init__(self, count):
        self.count = count
        self.bits = count.bit_length() - 1
        self.scatter_mask = [bit_reverse(count - 1 - p, self.bits) for p in range(count)]
        self.gather_mask = [bit_reverse(p, self.bits) for p in range(count)]

    def swap(self, array, bit):
        return lax.ppermute(array, "tp", [(i, i ^ (1 << bit)) for i in range(self.count)])

    def reduce_scatter(self, send, keep):
        for bit in range(self.bits):
            received = self.swap(send.astype(jnp.bfloat16), bit)
            held = keep.astype(jnp.float32) + received.astype(jnp.float32)
            half = held.shape[1] // 2
            send, keep = held[:, :half], held[:, half:]
        return held

    def gather(self, own):
        pieces = [own]
        for bit in reversed(range(self.bits)):
            held = pieces[0] if len(pieces) == 1 else jnp.concatenate(pieces, axis=1)
            pieces.append(self.swap(held, bit))
        return pieces


def softplus(v):
    return jnp.maximum(v, 0.0) + jnp.log1p(jnp.exp(-jnp.abs(v)))


def three(v, axis):
    high = v.astype(jnp.bfloat16)
    rest = v - high.astype(jnp.float32)
    mid = rest.astype(jnp.bfloat16)
    low = (rest - mid.astype(jnp.float32)).astype(jnp.bfloat16)
    return jnp.concatenate([high, mid, low], axis=axis)


def spread(v, width):
    heads = v.shape[1]
    high = v.astype(jnp.bfloat16)
    low = (v - high.astype(jnp.float32)).astype(jnp.bfloat16)
    row = lax.broadcasted_iota(jnp.int32, (2 * heads, heads * width), 0)
    column = lax.broadcasted_iota(jnp.int32, (2 * heads, heads * width), 1) // width
    pick = ((row == column) | (row - heads == column)).astype(jnp.float32).astype(jnp.bfloat16)
    return jnp.dot(
        jnp.concatenate([high, low], axis=1), pick, preferred_element_type=jnp.float32
    )


def decay_kernel(pre_ref, add_ref, rate_ref, rows_ref, cols_ref, scale_ref, last_ref):
    _, heads, length = pre_ref.shape
    width = scale_ref.shape[2] // heads
    at0 = lax.broadcasted_iota(jnp.int32, (length, length), 0)
    at1 = lax.broadcasted_iota(jnp.int32, (length, length), 1)
    steps, runs = [], []
    for way in range(2):
        reach = (at0 <= at1) if way == 0 else (at0 >= at1)
        reach = reach.astype(jnp.float32).astype(jnp.bfloat16)
        step = softplus(pre_ref[way])
        log = add_ref[way] - step * jnp.exp(rate_ref[:, way : way + 1])
        sums = jnp.dot(three(log, 0), reach, preferred_element_type=jnp.float32)
        run = sums[:heads] + sums[heads : 2 * heads] + sums[2 * heads :]
        rows_ref[way] = jnp.log(step) - run
        steps.append(step)
        runs.append(run)
    rows_ref[2] = jnp.log(steps[0] + steps[1])
    rest = jnp.zeros((128 - 4 * heads, length), jnp.float32)
    turned = jnp.concatenate([*runs, *steps, rest], axis=0).T
    for way in range(2):
        down = turned[:, way * heads : (way + 1) * heads]
        step = turned[:, (2 + way) * heads : (3 + way) * heads]
        end = down[length - 1 : length] if way == 0 else down[0:1]
        cols_ref[way] = down
        scale_ref[way] = spread(jnp.exp(end - down) * step, width)
        last_ref[way] = spread(jnp.broadcast_to(jnp.exp(end), (8, heads)), width)


def message(state, decay):
    high = decay.astype(jnp.bfloat16).astype(jnp.float32)
    low = decay - high
    row = lax.broadcasted_iota(jnp.int32, (TAIL, state.shape[1]), 0)
    tail = jnp.where(row == 0, high, jnp.where(row == 1, low, 0.0))
    return jnp.concatenate([state, tail], axis=0).astype(jnp.bfloat16)


def state_kernel(values_ref, inputs_ref, scale_ref, last_ref, window_ref, send_f_ref, send_b_ref):
    groups = inputs_ref.shape[1] // STATE
    wide = values_ref.shape[1] // groups
    values = values_ref[...].astype(jnp.float32)
    for way, send_ref in enumerate((send_f_ref, send_b_ref)):
        scaled = (values * scale_ref[way]).astype(jnp.bfloat16)
        state = jnp.concatenate(
            [
                lax.dot_general(
                    inputs_ref[:, g * STATE : (g + 1) * STATE],
                    scaled[:, g * wide : (g + 1) * wide],
                    (((0,), (0,)), ((), ())),
                    preferred_element_type=jnp.float32,
                )
                for g in range(groups)
            ],
            axis=1,
        )
        window_ref[way, :STATE] = state
        window_ref[way, STATE:] = last_ref[way]
        send_ref[...] = message(state, last_ref[way, 0:1])


def link_kernel(first, final, *refs):
    got_refs, refs = refs[:2], list(refs[2:])
    before_ref = None if first else refs.pop(0)
    window_ref = None if final else refs.pop(0)
    for way in range(2):
        got = got_refs[way][:STATE].astype(jnp.float32)
        got_decay = got_refs[way][STATE : STATE + 1].astype(jnp.float32) + got_refs[way][
            STATE + 1 : STATE + 2
        ].astype(jnp.float32)
        before, before_decay = got, got_decay
        if not first:
            held_decay = before_ref[way, STATE : STATE + 1]
            before = got * held_decay + before_ref[way, :STATE]
            before_decay = got_decay * held_decay
        if final:
            refs[0][way] = before.astype(jnp.bfloat16)
            continue
        decay = window_ref[way, STATE : STATE + 1]
        state = got * decay + window_ref[way, :STATE]
        decay = decay * got_decay
        for ref, value, factor in ((refs[0], before, before_decay), (refs[1], state, decay)):
            ref[way, :STATE] = value
            ref[way, STATE:] = jnp.broadcast_to(factor, (8, factor.shape[1]))
        refs[2 + way][...] = message(state, decay)


def within_kernel(values_ref, inputs_ref, readout_ref, rows_ref, cols_ref, out_ref):
    heads = rows_ref.shape[1]
    length = values_ref.shape[0]
    width = values_ref.shape[1] // heads
    tile = min(256, length)
    groups = inputs_ref.shape[1] // STATE
    per_group = heads // groups
    pack = max(1, 128 // width)
    lane = lax.broadcasted_iota(jnp.int32, (length, pack * width), 1) // width
    at0 = lax.broadcasted_iota(jnp.int32, (tile, tile), 0)
    at1 = lax.broadcasted_iota(jnp.int32, (tile, tile), 1)
    for g in range(groups):
        for i in range(length // tile):
            here = slice(i * tile, (i + 1) * tile)
            scores = lax.dot_general(
                readout_ref[here, g * STATE : (g + 1) * STATE],
                inputs_ref[:, g * STATE : (g + 1) * STATE],
                (((1,), (1,)), ((), ())),
                preferred_element_type=jnp.float32,
            )
            for first in range(0, per_group, pack):
                total = None
                channels = slice((g * per_group + first) * width, (g * per_group + first + pack) * width)
                packed = values_ref[:, channels]
                for sub in range(pack):
                    h = g * per_group + first + sub
                    own = jnp.where(lane == sub, packed, jnp.zeros_like(packed))
                    down_f = cols_ref[0, here, h : h + 1]
                    down_b = cols_ref[1, here, h : h + 1]
                    pieces = []
                    for j in range(length // tile):
                        there = slice(j * tile, (j + 1) * tile)
                        if i > j:
                            gap = down_f + rows_ref[0, h : h + 1, there]
                        elif i < j:
                            gap = down_b + rows_ref[1, h : h + 1, there]
                        else:
                            gap = jnp.where(
                                at0 > at1,
                                down_f + rows_ref[0, h : h + 1, there],
                                jnp.where(
                                    at0 < at1,
                                    down_b + rows_ref[1, h : h + 1, there],
                                    rows_ref[2, h : h + 1, there],
                                ),
                            )
                        pieces.append((scores[:, there] * jnp.exp(gap)).astype(jnp.bfloat16))
                    weights = jnp.concatenate(pieces, axis=1)
                    term = jnp.dot(weights, own, preferred_element_type=jnp.float32)
                    total = term if total is None else total + term
                out_ref[here, channels] = total


def close_kernel(sizes, info_ref, within_ref, readout_ref, cols_ref, states_ref, valve_ref, factor_ref, map_ref, send_ref, keep_ref):
    groups = readout_ref.shape[1] // STATE
    wide = within_ref.shape[1] // groups
    heads = cols_ref.shape[2]
    width = within_ref.shape[1] // heads
    lift_f = spread(jnp.exp(cols_ref[0]), width)
    lift_b = spread(jnp.exp(cols_ref[1]), width)
    blended = []
    for g in range(groups):
        at = slice(g * wide, (g + 1) * wide)
        readout = readout_ref[:, g * STATE : (g + 1) * STATE]
        carried_f = jnp.dot(readout, states_ref[0, :, at], preferred_element_type=jnp.float32)
        carried_b = jnp.dot(readout, states_ref[1, :, at], preferred_element_type=jnp.float32)
        mixed = within_ref[:, at] + carried_f * lift_f[:, at] + carried_b * lift_b[:, at]
        valve = valve_ref[:, at].astype(jnp.float32)
        gated = mixed * (valve / (1.0 + jnp.exp(-valve)))
        square = jnp.mean(gated * gated, axis=1, keepdims=True)
        scaled = gated * lax.rsqrt(square + EPSILON)
        blended.append((scaled * factor_ref[:, at]).astype(jnp.bfloat16))
    rows = jnp.concatenate(blended, axis=1)
    sp_count, count = sizes
    block = map_ref.shape[1] // count
    for p in range(count):
        columns = pl.ds(pl.multiple_of(info_ref[2 * sp_count + p] * block, block), block)
        term = jnp.dot(rows, map_ref[:, columns], preferred_element_type=jnp.float32).astype(jnp.bfloat16)
        target, at = (send_ref, p) if p < count // 2 else (keep_ref, p - count // 2)
        target[:, at * block : (at + 1) * block] = term


def up_kernel(sizes, plan, counts, last, *refs):
    n_pieces, n_arrays = counts
    sp_count, tp_count = sizes
    info_ref, gain_ref = refs[:2]
    pieces = refs[2 : 2 + n_pieces]
    arrays = refs[2 + n_pieces : 2 + n_pieces + n_arrays]
    outs = refs[2 + n_pieces + n_arrays : 4 + n_pieces + n_arrays]
    last_ref, rows_scr, gain_scr = refs[4 + n_pieces + n_arrays :]
    length, full = pieces[0].shape[0], gain_ref.shape[1]
    chunk, block = full // sp_count, full // tp_count
    for p in range(tp_count):
        at = pl.multiple_of(info_ref[2 * sp_count + tp_count + p] * block, block)
        gain_scr[:, p * block : (p + 1) * block] = gain_ref[:, pl.ds(at, block)]

    band = 64

    def norm(r, carry):
        rows = pl.ds(pl.multiple_of(r * band, band), band)
        parts = [piece[rows, :].astype(jnp.float32) for piece in pieces]
        square = sum(jnp.sum(part * part, axis=1, keepdims=True) for part in parts) / full
        factor = lax.rsqrt(square + EPSILON)
        start = 0
        for part in parts:
            for first in range(0, part.shape[1], chunk):
                at = start + first
                rows_scr[at // chunk, rows, :] = (
                    part[:, first : first + chunk] * factor * gain_scr[:, at : at + chunk]
                ).astype(jnp.bfloat16)
            start += part.shape[1]
        return carry

    lax.fori_loop(0, length // band, norm, 0)
    last_ref[...] = rows_scr[info_ref[last] // chunk]
    columns = outs[0].shape[1]
    tile = 256 if columns % 256 == 0 else columns
    for which in range(2):
        for j in range(columns // tile):
            at = slice(j * tile, (j + 1) * tile)
            total = None
            for n, source in enumerate(plan[which]):
                term = jnp.dot(
                    rows_scr[info_ref[source] // chunk],
                    arrays[which * len(plan[0]) + n][:, at],
                    preferred_element_type=jnp.float32,
                )
                total = term if total is None else total + term
            outs[which][:, at] = total


def up_last_kernel(gate_ref, value_ref, rows_ref, gate_map_ref, value_map_ref, gate_out, value_out):
    columns = gate_ref.shape[1]
    tile = 256 if columns % 256 == 0 else columns
    for held, map_ref, out in ((gate_ref, gate_map_ref, gate_out), (value_ref, value_map_ref, value_out)):
        for j in range(columns // tile):
            at = slice(j * tile, (j + 1) * tile)
            term = jnp.dot(rows_ref[...], map_ref[:, at], preferred_element_type=jnp.float32)
            out[:, at] = (held[:, at] + term).astype(jnp.bfloat16)


def down_kernel(sizes, plan, n_arrays, *refs):
    info_ref, hidden_ref = refs[:2]
    arrays = refs[2 : 2 + n_arrays]
    out_ref = refs[-1]
    for source, parts in plan:
        term = down_term(hidden_ref, [(arrays[array], row) for array, row in parts])
        out_ref[info_ref[sizes[0] + source] // term.shape[1]] = term


def down_last_kernel(sizes, plan, blank, rows, n_arrays, *refs):
    info_ref, hidden_ref, held_ref = refs[:3]
    arrays = refs[3 : 3 + n_arrays]
    outs = refs[-2:]
    count, _, chunk = held_ref.shape
    spots = [info_ref[sizes[0] + source] // chunk for source, _ in plan]
    terms = [down_term(hidden_ref.at[rows], [(arrays[array], row) for array, row in parts]) for _, parts in plan]
    spots.append(info_ref[sizes[0] + blank] // chunk)
    terms.append(jnp.zeros_like(terms[0]))
    for p in range(count):
        value = held_ref[p, rows]
        for spot, term in zip(spots, terms):
            value = jnp.where(spot == p, term, value)
        side, at = divmod(p * chunk, outs[0].shape[1])
        outs[side][:, at : at + chunk] = value


def down_whole_kernel(hidden_ref, map_ref, send_ref, keep_ref):
    half = send_ref.shape[1]
    for out_ref, first in ((send_ref, 0), (keep_ref, half)):
        out_ref[...] = down_term(hidden_ref, [(map_ref.at[:, first : first + half], 0)])


def down_term(hidden_ref, parts):
    term = None
    for array, row in parts:
        part = jnp.dot(
            hidden_ref[:, row : row + array.shape[0]], array[...], preferred_element_type=jnp.float32
        )
        term = part if term is None else term + part
    return term.astype(jnp.bfloat16)


def far_kernel(hidden_ref, top_ref, bottom_ref, out_ref):
    out_ref[...] = down_term(hidden_ref, [(top_ref, 0), (bottom_ref, top_ref.shape[0])])


def conv_rows(padded, kernel, length):
    summed = padded[0:length] * kernel[0]
    for offset in range(1, kernel.shape[0]):
        summed = summed + padded[offset : offset + length] * kernel[offset]
    return summed


def edges(last, first):
    count = lax.axis_size("sp")
    forward = [(i, i + 1) for i in range(count - 1)]
    backward = [(b, a) for a, b in forward]
    low = lax.ppermute(last, "sp", forward)
    high = lax.ppermute(first, "sp", backward)
    return low, high


def call(kernel, outs, *args, scalars=0, scratch=()):
    spaces = [pltpu.SMEM] * scalars + [pltpu.VMEM] * (len(args) - scalars)
    return pl.pallas_call(
        kernel,
        out_shape=[jax.ShapeDtypeStruct(shape, kind) for shape, kind in outs],
        in_specs=[pl.BlockSpec(memory_space=space) for space in spaces],
        scratch_shapes=list(scratch),
        compiler_params=pltpu.CompilerParams(vmem_limit_bytes=LIMIT * 1024 * 1024),
    )(*args)


def solution(mesh):
    cycle = ring_cycle(mesh)
    sp_count = mesh.shape["sp"]
    tp_count = mesh.shape["tp"]
    place = {s: i for i, s in enumerate(cycle)}
    right = [(cycle[i], cycle[(i + 1) % sp_count]) for i in range(sp_count)]
    left = [(b, a) for a, b in right]
    tp = Butterfly(tp_count)
    scatter_place = np.argsort(np.array(tp.scatter_mask))
    gather_place = np.argsort(np.array(tp.gather_mask))

    def table(chunk, own_cols):
        lines = []
        for s in range(sp_count):
            for t in range(tp_count):
                up, down = [], []
                for steps in range(sp_count):
                    block, rest = divmod(cycle[(place[s] - steps) % sp_count] * chunk, own_cols)
                    up.append(gather_place[block ^ t] * own_cols + rest)
                    down.append(scatter_place[block ^ t] * own_cols + rest)
                lines.append(up + down + [t ^ m for m in tp.scatter_mask] + [t ^ m for m in tp.gather_mask])
        return np.array(lines, np.int32)

    def send_on(array, pairs):
        return lax.ppermute(array, "sp", pairs)

    def ring(own, far_ways):
        out = []
        going, coming = own, own
        for step in range(1, (sp_count - 1) // 2 + 1):
            going = send_on(going, right)
            coming = send_on(coming, left)
            out += [(step, going, 0), (-step, coming, 0)]
        if sp_count % 2 == 0:
            far = sp_count // 2
            half = own.shape[0] // 2
            if far_ways == "f":
                out.append((far, send_on(going, right), 0))
            elif far_ways == "b":
                out.append((far, send_on(coming, left), 0))
            else:
                out.append((far, send_on(going[:half], right), 0))
                out.append((far, send_on(coming[half:], left), half))
        return out

    def shards(
        skip_trunk_vector,
        valve_preactivation,
        projected_heads_payload,
        cluster_ingests,
        cluster_observers,
        pre_softplus_increments,
        attenuation_ln_rate,
        additional_attenuation,
        payload_conv_weights,
        ingest_conv_weights,
        observer_conv_weights,
        valved_cluster_factor,
        closing_map_matrix,
        dense_standardize_factor,
        dense_valve_map,
        dense_payload_map,
        valve_series_smoother,
        payload_series_smoother,
        dense_contract_map,
    ):
        length = skip_trunk_vector.shape[0]
        heads = pre_softplus_increments.shape[2]
        channels = projected_heads_payload.shape[1]
        in_cols = cluster_ingests.shape[1]
        own_cols = skip_trunk_vector.shape[1]
        me = lax.axis_index("tp")

        margin = payload_conv_weights.shape[0] // 2
        streams = (projected_heads_payload, cluster_ingests, cluster_observers)
        low, high = edges(
            jnp.concatenate([a[length - margin :] for a in streams], axis=1),
            jnp.concatenate([a[:margin] for a in streams], axis=1),
        )

        full = own_cols * tp_count
        hidden_cols = dense_valve_map.shape[1]
        chunk = dense_valve_map.shape[0]
        up_rings = [[(0, own, 0)] + ring(own, way) for own, way in ((dense_valve_map, "f"), (dense_payload_map, "b"))]
        half_row = hidden_cols // 2
        down_rings = [
            [(0, own, 0)] + ring(own, way)
            for own, way in ((dense_contract_map[:half_row], "f"), (dense_contract_map[half_row:], "b"))
        ]
        info = jnp.asarray(table(chunk, own_cols))[lax.axis_index("sp") * tp_count + me]

        rows, cols, scale, last = call(
            decay_kernel,
            [
                ((3, heads, length), jnp.float32),
                ((2, length, heads), jnp.float32),
                ((2, length, channels), jnp.float32),
                ((2, 8, channels), jnp.float32),
            ],
            jnp.transpose(pre_softplus_increments, (0, 2, 1)),
            jnp.transpose(additional_attenuation, (0, 2, 1)),
            attenuation_ln_rate.T,
        )

        def mixed(array, low, high, kernel):
            padded = jnp.concatenate([low, array, high], axis=0).astype(jnp.float32)
            return jax.nn.silu(conv_rows(padded, kernel, length)).astype(jnp.bfloat16)

        ends = (channels, channels + in_cols)
        lows, highs = jnp.split(low, ends, axis=1), jnp.split(high, ends, axis=1)
        values = mixed(projected_heads_payload, lows[0], highs[0], payload_conv_weights)
        inputs = mixed(cluster_ingests, lows[1], highs[1], ingest_conv_weights)
        readout = mixed(cluster_observers, lows[2], highs[2], observer_conv_weights)
        wide_state = ((2, STATE + 8, channels), jnp.float32)
        sent = ((STATE + TAIL, channels), jnp.bfloat16)
        window, send_f, send_b = call(
            state_kernel, [wide_state, sent, sent], values, inputs, scale, last
        )
        (within,) = call(
            within_kernel, [((length, channels), jnp.float32)], values, inputs, readout, rows, cols
        )

        before, offset = (), 1
        while offset < sp_count:
            forward = [(i, i + offset) for i in range(sp_count - offset)]
            got_f = lax.ppermute(send_f, "sp", forward)
            got_b = lax.ppermute(send_b, "sp", [(b, a) for a, b in forward])
            final = 2 * offset >= sp_count
            outs = [((2, STATE, channels), jnp.bfloat16)]
            if not final:
                outs = [wide_state, wide_state, sent, sent]
            result = call(
                functools.partial(link_kernel, offset == 1, final),
                outs,
                got_f,
                got_b,
                *before,
                *(() if final else (window,)),
            )
            if final:
                states = result[0]
            else:
                before, (window, send_f, send_b) = (result[0],), result[1:]
            offset *= 2

        half_full = full // 2
        send, keep = call(
            functools.partial(close_kernel, (sp_count, tp_count)),
            [((length, half_full), jnp.bfloat16)] * 2,
            info,
            within,
            readout,
            cols,
            states,
            valve_preactivation,
            valved_cluster_factor[None, :],
            closing_map_matrix,
            scalars=1,
        )
        projected = tp.reduce_scatter(send, keep)
        middle = (skip_trunk_vector.astype(jnp.float32) + projected).astype(jnp.bfloat16)
        pieces = tp.gather(middle)

        arrays = [array for entries in up_rings for _, array, _ in entries[:-1]]
        plan = [[steps % sp_count for steps, _, _ in entries[:-1]] for entries in up_rings]
        last = up_rings[0][-1][0] % sp_count
        gate_sum, value_sum, last_rows = call(
            functools.partial(up_kernel, (sp_count, tp_count), plan, (len(pieces), len(arrays)), last),
            [((length, hidden_cols), jnp.float32)] * 2 + [((length, chunk), jnp.bfloat16)],
            info,
            dense_standardize_factor[None, :],
            *pieces,
            *arrays,
            scalars=1,
            scratch=[pltpu.VMEM((sp_count, length, chunk), jnp.bfloat16), pltpu.VMEM((1, full), jnp.float32)],
        )
        gate_rows, value_rows = call(
            up_last_kernel,
            [((length, hidden_cols), jnp.bfloat16)] * 2,
            gate_sum,
            value_sum,
            last_rows,
            *(entries[-1][1] for entries in up_rings),
        )
        margin = valve_series_smoother.shape[0] // 2
        low, high = edges(
            jnp.concatenate([gate_rows[length - margin :], value_rows[length - margin :]], axis=1),
            jnp.concatenate([gate_rows[:margin], value_rows[:margin]], axis=1),
        )

        def smooth(array, low, high, kernel):
            return conv_rows(jnp.concatenate([low, array, high], axis=0).astype(jnp.float32), kernel, length)

        gate = smooth(gate_rows, low[:, :hidden_cols], high[:, :hidden_cols], valve_series_smoother)
        value = smooth(value_rows, low[:, hidden_cols:], high[:, hidden_cols:], payload_series_smoother)
        hidden = (jax.nn.silu(gate) * value).astype(jnp.bfloat16)

        halves = [((length, half_full), jnp.bfloat16)] * 2
        if chunk % 128:
            whole = jnp.zeros((hidden_cols, full), jnp.bfloat16)
            for part, entries in enumerate(down_rings):
                for steps, array, _ in entries:
                    corner = (part * half_row, info[sp_count + steps % sp_count])
                    whole = lax.dynamic_update_slice(whole, array, corner)
            send, keep = call(down_whole_kernel, halves, hidden, whole)
            down_sum = tp.reduce_scatter(send, keep)
            return (middle.astype(jnp.float32) + down_sum).astype(jnp.bfloat16)

        far = sp_count // 2
        pairs = [
            (steps % sp_count, (top, bottom)) for (steps, top, _), (_, bottom, _) in zip(*down_rings) if abs(steps) < far
        ]

        def part_of(kernel, chunks, outs, *given):
            plan = [(slot, [(2 * n, 0), (2 * n + 1, half_row)]) for n, (slot, _) in enumerate(chunks)]
            arrays = [array for _, both_parts in chunks for array in both_parts]
            return call(kernel(plan, len(arrays)), outs, info, hidden, *given, *arrays, scalars=1)

        sizes = (sp_count, tp_count)
        (early,) = part_of(
            lambda plan, count: functools.partial(down_kernel, sizes, plan, count),
            pairs[:-2],
            [((sp_count, length, chunk), jnp.bfloat16)],
        )
        sums = []
        for band in range(2):
            rows = slice(band * length // 2, (band + 1) * length // 2)
            send, keep = part_of(
                lambda plan, count: functools.partial(down_last_kernel, sizes, plan, far, rows, count),
                pairs[-2:],
                [((length // 2, half_full), jnp.bfloat16)] * 2,
                early,
            )
            sums.append(tp.reduce_scatter(send, keep))
        down_sum = jnp.concatenate(sums, axis=0)
        (part,) = call(
            far_kernel, [((length, chunk), jnp.bfloat16)], hidden, *(entries[-1][1] for entries in down_rings)
        )
        for bit in range(tp.bits):
            pairs = []
            for s in range(sp_count):
                owner = cycle[(place[s] - far) % sp_count] * chunk // own_cols
                for t in range(tp_count):
                    apart = t ^ owner
                    if apart >> bit & 1 and apart % (1 << bit) == 0:
                        pairs.append((s * tp_count + t, s * tp_count + (t ^ (1 << bit))))
            received = lax.ppermute(part.astype(jnp.bfloat16), ("sp", "tp"), pairs)
            part = part.astype(jnp.float32) + received.astype(jnp.float32)
        at = info[sp_count + far] - (tp_count - 1) * own_cols
        spots = range(0, own_cols, chunk)
        placed = jnp.concatenate([jnp.where(at == spot, part, 0.0) for spot in spots], axis=1)
        return (middle.astype(jnp.float32) + down_sum + placed).astype(jnp.bfloat16)

    return jax.shard_map(
        shards,
        mesh=mesh,
        in_specs=(
            P("sp", "tp"),
            P("sp", "tp"),
            P("sp", "tp"),
            P("sp", "tp"),
            P("sp", "tp"),
            P(None, "sp", "tp"),
            P(None, "tp"),
            P(None, "sp", "tp"),
            P(None, "tp"),
            P(None, "tp"),
            P(None, "tp"),
            P("tp"),
            P("tp", None),
            P(),
            P("sp", "tp"),
            P("sp", "tp"),
            P(None, "tp"),
            P(None, "tp"),
            P("tp", "sp"),
        ),
        out_specs=P("sp", "tp"),
        check_vma=False,
    )
```

```python
import functools

import jax
import jax.numpy as jnp
import numpy as np
from jax import lax
from jax.experimental import pallas as pl
from jax.experimental.pallas import tpu as pltpu
from jax.sharding import PartitionSpec as P


STATE = 128
EPSILON = 1e-06
TAIL = 8
LIMIT = 16


def ring_cycle(mesh):
    line = mesh.devices[:, 0].ravel()
    count = len(line)
    if not all(hasattr(d, "coords") for d in line):
        return list(range(count))
    spots = {(d.coords[2], d.coords[1]): i for i, d in enumerate(line)}
    deep = sorted({z for z, _ in spots})
    wide = sorted({y for _, y in spots})
    if len(spots) != count or len(deep) % 2 or len(wide) < 2:
        return list(range(count))
    path = []
    for at, z in enumerate(deep):
        row = wide[1:] if at % 2 == 0 else wide[:0:-1]
        path += [(z, y) for y in row]
    path += [(z, wide[0]) for z in reversed(deep)]
    return [spots[spot] for spot in path]


def bit_reverse(value, bits):
    return int(format(value, f"0{bits}b")[::-1], 2) if bits else 0


class Butterfly:
    def __init__(self, count):
        self.count = count
        self.bits = count.bit_length() - 1
        self.scatter_mask = [bit_reverse(count - 1 - p, self.bits) for p in range(count)]
        self.gather_mask = [bit_reverse(p, self.bits) for p in range(count)]

    def swap(self, array, bit):
        return lax.ppermute(array, "tp", [(i, i ^ (1 << bit)) for i in range(self.count)])

    def reduce_scatter(self, send, keep):
        for bit in range(self.bits):
            received = self.swap(send.astype(jnp.bfloat16), bit)
            held = keep.astype(jnp.float32) + received.astype(jnp.float32)
            half = held.shape[1] // 2
            send, keep = held[:, :half], held[:, half:]
        return held

    def gather(self, own):
        pieces = [own]
        for bit in reversed(range(self.bits)):
            held = pieces[0] if len(pieces) == 1 else jnp.concatenate(pieces, axis=1)
            pieces.append(self.swap(held, bit))
        return pieces


def softplus(v):
    return jnp.maximum(v, 0.0) + jnp.log1p(jnp.exp(-jnp.abs(v)))


def three(v, axis):
    high = v.astype(jnp.bfloat16)
    rest = v - high.astype(jnp.float32)
    mid = rest.astype(jnp.bfloat16)
    low = (rest - mid.astype(jnp.float32)).astype(jnp.bfloat16)
    return jnp.concatenate([high, mid, low], axis=axis)


def spread(v, width):
    heads = v.shape[1]
    high = v.astype(jnp.bfloat16)
    low = (v - high.astype(jnp.float32)).astype(jnp.bfloat16)
    row = lax.broadcasted_iota(jnp.int32, (2 * heads, heads * width), 0)
    column = lax.broadcasted_iota(jnp.int32, (2 * heads, heads * width), 1) // width
    pick = ((row == column) | (row - heads == column)).astype(jnp.float32).astype(jnp.bfloat16)
    return jnp.dot(
        jnp.concatenate([high, low], axis=1), pick, preferred_element_type=jnp.float32
    )


def decay_kernel(pre_ref, add_ref, rate_ref, rows_ref, cols_ref, scale_ref, last_ref):
    _, heads, length = pre_ref.shape
    width = scale_ref.shape[2] // heads
    at0 = lax.broadcasted_iota(jnp.int32, (length, length), 0)
    at1 = lax.broadcasted_iota(jnp.int32, (length, length), 1)
    steps, runs = [], []
    for way in range(2):
        reach = (at0 <= at1) if way == 0 else (at0 >= at1)
        reach = reach.astype(jnp.float32).astype(jnp.bfloat16)
        step = softplus(pre_ref[way])
        log = add_ref[way] - step * jnp.exp(rate_ref[:, way : way + 1])
        sums = jnp.dot(three(log, 0), reach, preferred_element_type=jnp.float32)
        run = sums[:heads] + sums[heads : 2 * heads] + sums[2 * heads :]
        rows_ref[way] = jnp.log(step) - run
        steps.append(step)
        runs.append(run)
    rows_ref[2] = jnp.log(steps[0] + steps[1])
    rest = jnp.zeros((128 - 4 * heads, length), jnp.float32)
    turned = jnp.concatenate([*runs, *steps, rest], axis=0).T
    for way in range(2):
        down = turned[:, way * heads : (way + 1) * heads]
        step = turned[:, (2 + way) * heads : (3 + way) * heads]
        end = down[length - 1 : length] if way == 0 else down[0:1]
        cols_ref[way] = down
        scale_ref[way] = spread(jnp.exp(end - down) * step, width)
        last_ref[way] = spread(jnp.broadcast_to(jnp.exp(end), (8, heads)), width)


def message(state, decay):
    high = decay.astype(jnp.bfloat16).astype(jnp.float32)
    low = decay - high
    row = lax.broadcasted_iota(jnp.int32, (TAIL, state.shape[1]), 0)
    tail = jnp.where(row == 0, high, jnp.where(row == 1, low, 0.0))
    return jnp.concatenate([state, tail], axis=0).astype(jnp.bfloat16)


def state_kernel(values_ref, inputs_ref, scale_ref, last_ref, window_ref, send_f_ref, send_b_ref):
    groups = inputs_ref.shape[1] // STATE
    wide = values_ref.shape[1] // groups
    values = values_ref[...].astype(jnp.float32)
    for way, send_ref in enumerate((send_f_ref, send_b_ref)):
        scaled = (values * scale_ref[way]).astype(jnp.bfloat16)
        state = jnp.concatenate(
            [
                lax.dot_general(
                    inputs_ref[:, g * STATE : (g + 1) * STATE],
                    scaled[:, g * wide : (g + 1) * wide],
                    (((0,), (0,)), ((), ())),
                    preferred_element_type=jnp.float32,
                )
                for g in range(groups)
            ],
            axis=1,
        )
        window_ref[way, :STATE] = state
        window_ref[way, STATE:] = last_ref[way]
        send_ref[...] = message(state, last_ref[way, 0:1])


def link_kernel(first, final, *refs):
    got_refs, refs = refs[:2], list(refs[2:])
    before_ref = None if first else refs.pop(0)
    window_ref = None if final else refs.pop(0)
    for way in range(2):
        got = got_refs[way][:STATE].astype(jnp.float32)
        got_decay = got_refs[way][STATE : STATE + 1].astype(jnp.float32) + got_refs[way][
            STATE + 1 : STATE + 2
        ].astype(jnp.float32)
        before, before_decay = got, got_decay
        if not first:
            held_decay = before_ref[way, STATE : STATE + 1]
            before = got * held_decay + before_ref[way, :STATE]
            before_decay = got_decay * held_decay
        if final:
            refs[0][way] = before.astype(jnp.bfloat16)
            continue
        decay = window_ref[way, STATE : STATE + 1]
        state = got * decay + window_ref[way, :STATE]
        decay = decay * got_decay
        for ref, value, factor in ((refs[0], before, before_decay), (refs[1], state, decay)):
            ref[way, :STATE] = value
            ref[way, STATE:] = jnp.broadcast_to(factor, (8, factor.shape[1]))
        refs[2 + way][...] = message(state, decay)


def within_kernel(values_ref, inputs_ref, readout_ref, rows_ref, cols_ref, out_ref):
    heads = rows_ref.shape[1]
    length = values_ref.shape[0]
    width = values_ref.shape[1] // heads
    tile = min(256, length)
    groups = inputs_ref.shape[1] // STATE
    per_group = heads // groups
    pack = max(1, 128 // width)
    lane = lax.broadcasted_iota(jnp.int32, (length, pack * width), 1) // width
    at0 = lax.broadcasted_iota(jnp.int32, (tile, tile), 0)
    at1 = lax.broadcasted_iota(jnp.int32, (tile, tile), 1)
    for g in range(groups):
        for i in range(length // tile):
            here = slice(i * tile, (i + 1) * tile)
            scores = lax.dot_general(
                readout_ref[here, g * STATE : (g + 1) * STATE],
                inputs_ref[:, g * STATE : (g + 1) * STATE],
                (((1,), (1,)), ((), ())),
                preferred_element_type=jnp.float32,
            )
            for first in range(0, per_group, pack):
                total = None
                channels = slice((g * per_group + first) * width, (g * per_group + first + pack) * width)
                packed = values_ref[:, channels]
                for sub in range(pack):
                    h = g * per_group + first + sub
                    own = jnp.where(lane == sub, packed, jnp.zeros_like(packed))
                    down_f = cols_ref[0, here, h : h + 1]
                    down_b = cols_ref[1, here, h : h + 1]
                    pieces = []
                    for j in range(length // tile):
                        there = slice(j * tile, (j + 1) * tile)
                        if i > j:
                            gap = down_f + rows_ref[0, h : h + 1, there]
                        elif i < j:
                            gap = down_b + rows_ref[1, h : h + 1, there]
                        else:
                            gap = jnp.where(
                                at0 > at1,
                                down_f + rows_ref[0, h : h + 1, there],
                                jnp.where(
                                    at0 < at1,
                                    down_b + rows_ref[1, h : h + 1, there],
                                    rows_ref[2, h : h + 1, there],
                                ),
                            )
                        pieces.append((scores[:, there] * jnp.exp(gap)).astype(jnp.bfloat16))
                    weights = jnp.concatenate(pieces, axis=1)
                    term = jnp.dot(weights, own, preferred_element_type=jnp.float32)
                    total = term if total is None else total + term
                out_ref[here, channels] = total


def close_kernel(sizes, info_ref, within_ref, readout_ref, cols_ref, states_ref, valve_ref, factor_ref, map_ref, send_ref, keep_ref):
    groups = readout_ref.shape[1] // STATE
    wide = within_ref.shape[1] // groups
    heads = cols_ref.shape[2]
    width = within_ref.shape[1] // heads
    lift_f = spread(jnp.exp(cols_ref[0]), width)
    lift_b = spread(jnp.exp(cols_ref[1]), width)
    blended = []
    for g in range(groups):
        at = slice(g * wide, (g + 1) * wide)
        readout = readout_ref[:, g * STATE : (g + 1) * STATE]
        carried_f = jnp.dot(readout, states_ref[0, :, at], preferred_element_type=jnp.float32)
        carried_b = jnp.dot(readout, states_ref[1, :, at], preferred_element_type=jnp.float32)
        mixed = within_ref[:, at] + carried_f * lift_f[:, at] + carried_b * lift_b[:, at]
        valve = valve_ref[:, at].astype(jnp.float32)
        gated = mixed * (valve / (1.0 + jnp.exp(-valve)))
        square = jnp.mean(gated * gated, axis=1, keepdims=True)
        scaled = gated * lax.rsqrt(square + EPSILON)
        blended.append((scaled * factor_ref[:, at]).astype(jnp.bfloat16))
    rows = jnp.concatenate(blended, axis=1)
    sp_count, count = sizes
    block = map_ref.shape[1] // count
    for p in range(count):
        columns = pl.ds(pl.multiple_of(info_ref[2 * sp_count + p] * block, block), block)
        term = jnp.dot(rows, map_ref[:, columns], preferred_element_type=jnp.float32).astype(jnp.bfloat16)
        target, at = (send_ref, p) if p < count // 2 else (keep_ref, p - count // 2)
        target[:, at * block : (at + 1) * block] = term


def up_kernel(sizes, plan, counts, last, *refs):
    n_pieces, n_arrays = counts
    sp_count, tp_count = sizes
    info_ref, gain_ref = refs[:2]
    pieces = refs[2 : 2 + n_pieces]
    arrays = refs[2 + n_pieces : 2 + n_pieces + n_arrays]
    outs = refs[2 + n_pieces + n_arrays : 4 + n_pieces + n_arrays]
    last_ref, rows_scr, gain_scr = refs[4 + n_pieces + n_arrays :]
    length, full = pieces[0].shape[0], gain_ref.shape[1]
    chunk, block = full // sp_count, full // tp_count
    for p in range(tp_count):
        at = pl.multiple_of(info_ref[2 * sp_count + tp_count + p] * block, block)
        gain_scr[:, p * block : (p + 1) * block] = gain_ref[:, pl.ds(at, block)]

    band = 64

    def norm(r, carry):
        rows = pl.ds(pl.multiple_of(r * band, band), band)
        parts = [piece[rows, :].astype(jnp.float32) for piece in pieces]
        square = sum(jnp.sum(part * part, axis=1, keepdims=True) for part in parts) / full
        factor = lax.rsqrt(square + EPSILON)
        start = 0
        for part in parts:
            for first in range(0, part.shape[1], chunk):
                at = start + first
                rows_scr[at // chunk, rows, :] = (
                    part[:, first : first + chunk] * factor * gain_scr[:, at : at + chunk]
                ).astype(jnp.bfloat16)
            start += part.shape[1]
        return carry

    lax.fori_loop(0, length // band, norm, 0)
    last_ref[...] = rows_scr[info_ref[last] // chunk]
    columns = outs[0].shape[1]
    tile = 256 if columns % 256 == 0 else columns
    for which in range(2):
        for j in range(columns // tile):
            at = slice(j * tile, (j + 1) * tile)
            total = None
            for n, source in enumerate(plan[which]):
                term = jnp.dot(
                    rows_scr[info_ref[source] // chunk],
                    arrays[which * len(plan[0]) + n][:, at],
                    preferred_element_type=jnp.float32,
                )
                total = term if total is None else total + term
            outs[which][:, at] = total


def up_last_kernel(gate_ref, value_ref, rows_ref, gate_map_ref, value_map_ref, gate_out, value_out):
    columns = gate_ref.shape[1]
    tile = 256 if columns % 256 == 0 else columns
    for held, map_ref, out in ((gate_ref, gate_map_ref, gate_out), (value_ref, value_map_ref, value_out)):
        for j in range(columns // tile):
            at = slice(j * tile, (j + 1) * tile)
            term = jnp.dot(rows_ref[...], map_ref[:, at], preferred_element_type=jnp.float32)
            out[:, at] = (held[:, at] + term).astype(jnp.bfloat16)


def down_kernel(sizes, plan, *refs):
    info_ref, hidden_ref = refs[:2]
    arrays, out_ref = refs[2:-1], refs[-1]
    for n, source in enumerate(plan):
        term = down_term(hidden_ref, arrays[2 * n : 2 * n + 2])
        out_ref[info_ref[sizes[0] + source] // term.shape[1]] = term


def down_last_kernel(sizes, plan, blank, band, *refs):
    info_ref, hidden_ref, held_ref = refs[:3]
    arrays, outs = refs[3:-2], refs[-2:]
    count, width = held_ref.shape[0], arrays[0].shape[1]
    columns = slice(band * width, (band + 1) * width)
    both_terms = down_term(hidden_ref, arrays)
    spots = [info_ref[sizes[0] + source] // held_ref.shape[2] for source in plan]
    terms = [both_terms[:, n * width : (n + 1) * width] for n in range(len(plan))]
    spots.append(info_ref[sizes[0] + blank] // held_ref.shape[2])
    terms.append(jnp.zeros_like(terms[0]))
    for p in range(count):
        value = held_ref[p, :, columns]
        for spot, term in zip(spots, terms):
            value = jnp.where(spot == p, term, value)
        side, at = divmod(p * width, outs[0].shape[1])
        outs[side][:, at : at + width] = value


def down_whole_kernel(hidden_ref, map_ref, send_ref, keep_ref):
    half = send_ref.shape[1]
    for out_ref, first in ((send_ref, 0), (keep_ref, half)):
        out_ref[...] = down_term(hidden_ref, [map_ref.at[:, first : first + half]])


def down_term(hidden_ref, parts):
    side_by_side = [part[...] for part in parts]
    whole = side_by_side[0] if len(parts) == 1 else jnp.concatenate(side_by_side, axis=1)
    return jnp.dot(hidden_ref[...], whole, preferred_element_type=jnp.float32).astype(jnp.bfloat16)


def far_kernel(hidden_ref, left_ref, right_ref, out_ref):
    out_ref[...] = down_term(hidden_ref, [left_ref, right_ref])


def conv_rows(padded, kernel, length):
    summed = padded[0:length] * kernel[0]
    for offset in range(1, kernel.shape[0]):
        summed = summed + padded[offset : offset + length] * kernel[offset]
    return summed


def edges(last, first):
    count = lax.axis_size("sp")
    forward = [(i, i + 1) for i in range(count - 1)]
    backward = [(b, a) for a, b in forward]
    low = lax.ppermute(last, "sp", forward)
    high = lax.ppermute(first, "sp", backward)
    return low, high


def call(kernel, outs, *args, scalars=0, scratch=()):
    spaces = [pltpu.SMEM] * scalars + [pltpu.VMEM] * (len(args) - scalars)
    return pl.pallas_call(
        kernel,
        out_shape=[jax.ShapeDtypeStruct(shape, kind) for shape, kind in outs],
        in_specs=[pl.BlockSpec(memory_space=space) for space in spaces],
        scratch_shapes=list(scratch),
        compiler_params=pltpu.CompilerParams(vmem_limit_bytes=LIMIT * 1024 * 1024),
    )(*args)


def solution(mesh):
    cycle = ring_cycle(mesh)
    sp_count = mesh.shape["sp"]
    tp_count = mesh.shape["tp"]
    place = {s: i for i, s in enumerate(cycle)}
    right = [(cycle[i], cycle[(i + 1) % sp_count]) for i in range(sp_count)]
    left = [(b, a) for a, b in right]
    tp = Butterfly(tp_count)
    scatter_place = np.argsort(np.array(tp.scatter_mask))
    gather_place = np.argsort(np.array(tp.gather_mask))

    def table(chunk, own_cols):
        lines = []
        for s in range(sp_count):
            for t in range(tp_count):
                up, down = [], []
                for steps in range(sp_count):
                    block, rest = divmod(cycle[(place[s] - steps) % sp_count] * chunk, own_cols)
                    up.append(gather_place[block ^ t] * own_cols + rest)
                    down.append(scatter_place[block ^ t] * own_cols + rest)
                lines.append(up + down + [t ^ m for m in tp.scatter_mask] + [t ^ m for m in tp.gather_mask])
        return np.array(lines, np.int32)

    def send_on(array, pairs):
        return lax.ppermute(array, "sp", pairs)

    def ring(own, far_ways):
        out = []
        going, coming = own, own
        for step in range(1, (sp_count - 1) // 2 + 1):
            going = send_on(going, right)
            coming = send_on(coming, left)
            out += [(step, going, 0), (-step, coming, 0)]
        if sp_count % 2 == 0:
            far = sp_count // 2
            half = own.shape[0] // 2
            if far_ways == "f":
                out.append((far, send_on(going, right), 0))
            elif far_ways == "b":
                out.append((far, send_on(coming, left), 0))
            else:
                out.append((far, send_on(going[:half], right), 0))
                out.append((far, send_on(coming[half:], left), half))
        return out

    def shards(
        skip_trunk_vector,
        valve_preactivation,
        projected_heads_payload,
        cluster_ingests,
        cluster_observers,
        pre_softplus_increments,
        attenuation_ln_rate,
        additional_attenuation,
        payload_conv_weights,
        ingest_conv_weights,
        observer_conv_weights,
        valved_cluster_factor,
        closing_map_matrix,
        dense_standardize_factor,
        dense_valve_map,
        dense_payload_map,
        valve_series_smoother,
        payload_series_smoother,
        dense_contract_map,
    ):
        length = skip_trunk_vector.shape[0]
        heads = pre_softplus_increments.shape[2]
        channels = projected_heads_payload.shape[1]
        in_cols = cluster_ingests.shape[1]
        own_cols = skip_trunk_vector.shape[1]
        me = lax.axis_index("tp")

        margin = payload_conv_weights.shape[0] // 2
        streams = (projected_heads_payload, cluster_ingests, cluster_observers)
        low, high = edges(
            jnp.concatenate([a[length - margin :] for a in streams], axis=1),
            jnp.concatenate([a[:margin] for a in streams], axis=1),
        )

        full = own_cols * tp_count
        hidden_cols = dense_valve_map.shape[1]
        chunk = dense_valve_map.shape[0]
        up_rings = [[(0, own, 0)] + ring(own, way) for own, way in ((dense_valve_map, "f"), (dense_payload_map, "b"))]
        half_col = chunk // 2
        down_rings = [
            [(0, own, 0)] + ring(own, way)
            for own, way in ((dense_contract_map[:, :half_col], "f"), (dense_contract_map[:, half_col:], "b"))
        ]
        info = jnp.asarray(table(chunk, own_cols))[lax.axis_index("sp") * tp_count + me]

        rows, cols, scale, last = call(
            decay_kernel,
            [
                ((3, heads, length), jnp.float32),
                ((2, length, heads), jnp.float32),
                ((2, length, channels), jnp.float32),
                ((2, 8, channels), jnp.float32),
            ],
            jnp.transpose(pre_softplus_increments, (0, 2, 1)),
            jnp.transpose(additional_attenuation, (0, 2, 1)),
            attenuation_ln_rate.T,
        )

        def mixed(array, low, high, kernel):
            padded = jnp.concatenate([low, array, high], axis=0).astype(jnp.float32)
            return jax.nn.silu(conv_rows(padded, kernel, length)).astype(jnp.bfloat16)

        ends = (channels, channels + in_cols)
        lows, highs = jnp.split(low, ends, axis=1), jnp.split(high, ends, axis=1)
        values = mixed(projected_heads_payload, lows[0], highs[0], payload_conv_weights)
        inputs = mixed(cluster_ingests, lows[1], highs[1], ingest_conv_weights)
        readout = mixed(cluster_observers, lows[2], highs[2], observer_conv_weights)
        wide_state = ((2, STATE + 8, channels), jnp.float32)
        sent = ((STATE + TAIL, channels), jnp.bfloat16)
        window, send_f, send_b = call(
            state_kernel, [wide_state, sent, sent], values, inputs, scale, last
        )
        (within,) = call(
            within_kernel, [((length, channels), jnp.float32)], values, inputs, readout, rows, cols
        )

        before, offset = (), 1
        while offset < sp_count:
            forward = [(i, i + offset) for i in range(sp_count - offset)]
            got_f = lax.ppermute(send_f, "sp", forward)
            got_b = lax.ppermute(send_b, "sp", [(b, a) for a, b in forward])
            final = 2 * offset >= sp_count
            outs = [((2, STATE, channels), jnp.bfloat16)]
            if not final:
                outs = [wide_state, wide_state, sent, sent]
            result = call(
                functools.partial(link_kernel, offset == 1, final),
                outs,
                got_f,
                got_b,
                *before,
                *(() if final else (window,)),
            )
            if final:
                states = result[0]
            else:
                before, (window, send_f, send_b) = (result[0],), result[1:]
            offset *= 2

        half_full = full // 2
        send, keep = call(
            functools.partial(close_kernel, (sp_count, tp_count)),
            [((length, half_full), jnp.bfloat16)] * 2,
            info,
            within,
            readout,
            cols,
            states,
            valve_preactivation,
            valved_cluster_factor[None, :],
            closing_map_matrix,
            scalars=1,
        )
        projected = tp.reduce_scatter(send, keep)
        middle = (skip_trunk_vector.astype(jnp.float32) + projected).astype(jnp.bfloat16)
        pieces = tp.gather(middle)

        arrays = [array for entries in up_rings for _, array, _ in entries[:-1]]
        plan = [[steps % sp_count for steps, _, _ in entries[:-1]] for entries in up_rings]
        last = up_rings[0][-1][0] % sp_count
        gate_sum, value_sum, last_rows = call(
            functools.partial(up_kernel, (sp_count, tp_count), plan, (len(pieces), len(arrays)), last),
            [((length, hidden_cols), jnp.float32)] * 2 + [((length, chunk), jnp.bfloat16)],
            info,
            dense_standardize_factor[None, :],
            *pieces,
            *arrays,
            scalars=1,
            scratch=[pltpu.VMEM((sp_count, length, chunk), jnp.bfloat16), pltpu.VMEM((1, full), jnp.float32)],
        )
        gate_rows, value_rows = call(
            up_last_kernel,
            [((length, hidden_cols), jnp.bfloat16)] * 2,
            gate_sum,
            value_sum,
            last_rows,
            *(entries[-1][1] for entries in up_rings),
        )
        margin = valve_series_smoother.shape[0] // 2
        low, high = edges(
            jnp.concatenate([gate_rows[length - margin :], value_rows[length - margin :]], axis=1),
            jnp.concatenate([gate_rows[:margin], value_rows[:margin]], axis=1),
        )

        def smooth(array, low, high, kernel):
            return conv_rows(jnp.concatenate([low, array, high], axis=0).astype(jnp.float32), kernel, length)

        gate = smooth(gate_rows, low[:, :hidden_cols], high[:, :hidden_cols], valve_series_smoother)
        value = smooth(value_rows, low[:, hidden_cols:], high[:, hidden_cols:], payload_series_smoother)
        hidden = (jax.nn.silu(gate) * value).astype(jnp.bfloat16)

        halves = [((length, half_full), jnp.bfloat16)] * 2
        if chunk % 256:
            whole = jnp.zeros((hidden_cols, full), jnp.bfloat16)
            for part, entries in enumerate(down_rings):
                for steps, array, _ in entries:
                    corner = (0, info[sp_count + steps % sp_count] + part * half_col)
                    whole = lax.dynamic_update_slice(whole, array, corner)
            send, keep = call(down_whole_kernel, halves, hidden, whole)
            down_sum = tp.reduce_scatter(send, keep)
            return (middle.astype(jnp.float32) + down_sum).astype(jnp.bfloat16)

        far = sp_count // 2
        near_steps = [steps for steps, _, _ in down_rings[0][:-1]]
        held_by = [[array for _, array, _ in entries[:-1]] for entries in down_rings]
        plan = [steps % sp_count for steps in near_steps]
        sizes = (sp_count, tp_count)
        (early,) = call(
            functools.partial(down_kernel, sizes, plan[:-2]),
            [((sp_count, length, chunk), jnp.bfloat16)],
            info,
            hidden,
            *(array for pair in list(zip(*held_by))[:-2] for array in pair),
            scalars=1,
        )
        sums = []
        for band in range(2):
            send, keep = call(
                functools.partial(down_last_kernel, sizes, plan[-2:], far, band),
                [((length, half_full // 2), jnp.bfloat16)] * 2,
                info,
                hidden,
                early,
                *held_by[band][-2:],
                scalars=1,
            )
            sums.append(tp.reduce_scatter(send, keep))
        down_sum = jnp.concatenate(
            [
                band[:, at : at + half_col]
                for at in range(0, own_cols // 2, half_col)
                for band in sums
            ],
            axis=1,
        )
        (part,) = call(
            far_kernel, [((length, chunk), jnp.bfloat16)], hidden, *(entries[-1][1] for entries in down_rings)
        )
        for bit in range(tp.bits):
            pairs = []
            for s in range(sp_count):
                owner = cycle[(place[s] - far) % sp_count] * chunk // own_cols
                for t in range(tp_count):
                    apart = t ^ owner
                    if apart >> bit & 1 and apart % (1 << bit) == 0:
                        pairs.append((s * tp_count + t, s * tp_count + (t ^ (1 << bit))))
            if bit == 0:
                received = tp.swap(part, bit)
            else:
                received = lax.ppermute(part.astype(jnp.bfloat16), ("sp", "tp"), pairs)
            part = part.astype(jnp.float32) + received.astype(jnp.float32)
        at = info[sp_count + far] - (tp_count - 1) * own_cols
        spots = range(0, own_cols, chunk)
        placed = jnp.concatenate([jnp.where(at == spot, part, 0.0) for spot in spots], axis=1)
        return (middle.astype(jnp.float32) + down_sum + placed).astype(jnp.bfloat16)

    return jax.shard_map(
        shards,
        mesh=mesh,
        in_specs=(
            P("sp", "tp"),
            P("sp", "tp"),
            P("sp", "tp"),
            P("sp", "tp"),
            P("sp", "tp"),
            P(None, "sp", "tp"),
            P(None, "tp"),
            P(None, "sp", "tp"),
            P(None, "tp"),
            P(None, "tp"),
            P(None, "tp"),
            P("tp"),
            P("tp", None),
            P(),
            P("sp", "tp"),
            P("sp", "tp"),
            P(None, "tp"),
            P(None, "tp"),
            P("tp", "sp"),
        ),
        out_specs=P("sp", "tp"),
        check_vma=False,
    )
```

```python
import functools

import jax
import jax.numpy as jnp
import numpy as np
from jax import lax
from jax.experimental import pallas as pl
from jax.experimental.pallas import tpu as pltpu
from jax.sharding import PartitionSpec as P


STATE = 128
EPSILON = 1e-06
TAIL = 8
LIMIT = 16


def ring_cycle(mesh):
    line = mesh.devices[:, 0].ravel()
    count = len(line)
    if not all(hasattr(d, "coords") for d in line):
        return list(range(count))
    spots = {(d.coords[2], d.coords[1]): i for i, d in enumerate(line)}
    deep = sorted({z for z, _ in spots})
    wide = sorted({y for _, y in spots})
    if len(spots) != count or len(deep) % 2 or len(wide) < 2:
        return list(range(count))
    path = []
    for at, z in enumerate(deep):
        row = wide[1:] if at % 2 == 0 else wide[:0:-1]
        path += [(z, y) for y in row]
    path += [(z, wide[0]) for z in reversed(deep)]
    return [spots[spot] for spot in path]


def bit_reverse(value, bits):
    return int(format(value, f"0{bits}b")[::-1], 2) if bits else 0


class Butterfly:
    def __init__(self, count):
        self.count = count
        self.bits = count.bit_length() - 1
        self.scatter_mask = [bit_reverse(count - 1 - p, self.bits) for p in range(count)]
        self.gather_mask = [bit_reverse(p, self.bits) for p in range(count)]

    def swap(self, array, bit):
        return lax.ppermute(array, "tp", [(i, i ^ (1 << bit)) for i in range(self.count)])

    def reduce_scatter(self, send, keep):
        for bit in range(self.bits):
            received = self.swap(send.astype(jnp.bfloat16), bit)
            held = keep.astype(jnp.float32) + received.astype(jnp.float32)
            half = held.shape[1] // 2
            send, keep = held[:, :half], held[:, half:]
        return held

    def gather(self, own):
        pieces = [own]
        for bit in reversed(range(self.bits)):
            held = pieces[0] if len(pieces) == 1 else jnp.concatenate(pieces, axis=1)
            pieces.append(self.swap(held, bit))
        return pieces


def softplus(v):
    return jnp.maximum(v, 0.0) + jnp.log1p(jnp.exp(-jnp.abs(v)))


def three(v, axis):
    high = v.astype(jnp.bfloat16)
    rest = v - high.astype(jnp.float32)
    mid = rest.astype(jnp.bfloat16)
    low = (rest - mid.astype(jnp.float32)).astype(jnp.bfloat16)
    return jnp.concatenate([high, mid, low], axis=axis)


def spread(v, width):
    heads = v.shape[1]
    high = v.astype(jnp.bfloat16)
    low = (v - high.astype(jnp.float32)).astype(jnp.bfloat16)
    row = lax.broadcasted_iota(jnp.int32, (2 * heads, heads * width), 0)
    column = lax.broadcasted_iota(jnp.int32, (2 * heads, heads * width), 1) // width
    pick = ((row == column) | (row - heads == column)).astype(jnp.float32).astype(jnp.bfloat16)
    return jnp.dot(
        jnp.concatenate([high, low], axis=1), pick, preferred_element_type=jnp.float32
    )


def decay_kernel(pre_ref, add_ref, rate_ref, rows_ref, cols_ref, scale_ref, last_ref):
    _, heads, length = pre_ref.shape
    width = scale_ref.shape[2] // heads
    at0 = lax.broadcasted_iota(jnp.int32, (length, length), 0)
    at1 = lax.broadcasted_iota(jnp.int32, (length, length), 1)
    steps, runs = [], []
    for way in range(2):
        reach = (at0 <= at1) if way == 0 else (at0 >= at1)
        reach = reach.astype(jnp.float32).astype(jnp.bfloat16)
        step = softplus(pre_ref[way])
        log = add_ref[way] - step * jnp.exp(rate_ref[:, way : way + 1])
        sums = jnp.dot(three(log, 0), reach, preferred_element_type=jnp.float32)
        run = sums[:heads] + sums[heads : 2 * heads] + sums[2 * heads :]
        rows_ref[way] = jnp.log(step) - run
        steps.append(step)
        runs.append(run)
    rows_ref[2] = jnp.log(steps[0] + steps[1])
    rest = jnp.zeros((128 - 4 * heads, length), jnp.float32)
    turned = jnp.concatenate([*runs, *steps, rest], axis=0).T
    for way in range(2):
        down = turned[:, way * heads : (way + 1) * heads]
        step = turned[:, (2 + way) * heads : (3 + way) * heads]
        end = down[length - 1 : length] if way == 0 else down[0:1]
        cols_ref[way] = down
        scale_ref[way] = spread(jnp.exp(end - down) * step, width)
        last_ref[way] = spread(jnp.broadcast_to(jnp.exp(end), (8, heads)), width)


def message(state, decay):
    high = decay.astype(jnp.bfloat16).astype(jnp.float32)
    low = decay - high
    row = lax.broadcasted_iota(jnp.int32, (TAIL, state.shape[1]), 0)
    tail = jnp.where(row == 0, high, jnp.where(row == 1, low, 0.0))
    return jnp.concatenate([state, tail], axis=0).astype(jnp.bfloat16)


def state_kernel(values_ref, inputs_ref, scale_ref, last_ref, window_ref, send_f_ref, send_b_ref):
    groups = inputs_ref.shape[1] // STATE
    wide = values_ref.shape[1] // groups
    values = values_ref[...].astype(jnp.float32)
    for way, send_ref in enumerate((send_f_ref, send_b_ref)):
        scaled = (values * scale_ref[way]).astype(jnp.bfloat16)
        state = jnp.concatenate(
            [
                lax.dot_general(
                    inputs_ref[:, g * STATE : (g + 1) * STATE],
                    scaled[:, g * wide : (g + 1) * wide],
                    (((0,), (0,)), ((), ())),
                    preferred_element_type=jnp.float32,
                )
                for g in range(groups)
            ],
            axis=1,
        )
        window_ref[way, :STATE] = state
        window_ref[way, STATE:] = last_ref[way]
        send_ref[...] = message(state, last_ref[way, 0:1])


def link_kernel(first, final, *refs):
    got_refs, refs = refs[:2], list(refs[2:])
    before_ref = None if first else refs.pop(0)
    window_ref = None if final else refs.pop(0)
    for way in range(2):
        got = got_refs[way][:STATE].astype(jnp.float32)
        before = got
        if not first:
            held_decay = before_ref[way, STATE : STATE + 1]
            before = got * held_decay + before_ref[way, :STATE]
        if final:
            refs[0][way] = before.astype(jnp.bfloat16)
            continue
        got_decay = got_refs[way][STATE : STATE + 1].astype(jnp.float32) + got_refs[way][
            STATE + 1 : STATE + 2
        ].astype(jnp.float32)
        before_decay = got_decay if first else got_decay * held_decay
        decay = window_ref[way, STATE : STATE + 1]
        state = got * decay + window_ref[way, :STATE]
        decay = decay * got_decay
        for ref, value, factor in ((refs[0], before, before_decay), (refs[1], state, decay)):
            ref[way, :STATE] = value
            ref[way, STATE:] = jnp.broadcast_to(factor, (8, factor.shape[1]))
        alone = refs[2 + way].shape[0] == STATE
        refs[2 + way][...] = state.astype(jnp.bfloat16) if alone else message(state, decay)


def within_kernel(values_ref, inputs_ref, readout_ref, rows_ref, cols_ref, out_ref):
    heads = rows_ref.shape[1]
    length = values_ref.shape[0]
    width = values_ref.shape[1] // heads
    tile = min(256, length)
    groups = inputs_ref.shape[1] // STATE
    per_group = heads // groups
    pack = max(1, 128 // width)
    lane = lax.broadcasted_iota(jnp.int32, (length, pack * width), 1) // width
    at0 = lax.broadcasted_iota(jnp.int32, (tile, tile), 0)
    at1 = lax.broadcasted_iota(jnp.int32, (tile, tile), 1)
    for g in range(groups):
        for i in range(length // tile):
            here = slice(i * tile, (i + 1) * tile)
            scores = lax.dot_general(
                readout_ref[here, g * STATE : (g + 1) * STATE],
                inputs_ref[:, g * STATE : (g + 1) * STATE],
                (((1,), (1,)), ((), ())),
                preferred_element_type=jnp.float32,
            )
            for first in range(0, per_group, pack):
                total = None
                channels = slice((g * per_group + first) * width, (g * per_group + first + pack) * width)
                packed = values_ref[:, channels]
                for sub in range(pack):
                    h = g * per_group + first + sub
                    own = jnp.where(lane == sub, packed, jnp.zeros_like(packed))
                    down_f = cols_ref[0, here, h : h + 1]
                    down_b = cols_ref[1, here, h : h + 1]
                    pieces = []
                    for j in range(length // tile):
                        there = slice(j * tile, (j + 1) * tile)
                        if i > j:
                            gap = down_f + rows_ref[0, h : h + 1, there]
                        elif i < j:
                            gap = down_b + rows_ref[1, h : h + 1, there]
                        else:
                            gap = jnp.where(
                                at0 > at1,
                                down_f + rows_ref[0, h : h + 1, there],
                                jnp.where(
                                    at0 < at1,
                                    down_b + rows_ref[1, h : h + 1, there],
                                    rows_ref[2, h : h + 1, there],
                                ),
                            )
                        pieces.append((scores[:, there] * jnp.exp(gap)).astype(jnp.bfloat16))
                    weights = jnp.concatenate(pieces, axis=1)
                    term = jnp.dot(weights, own, preferred_element_type=jnp.float32)
                    total = term if total is None else total + term
                out_ref[here, channels] = total


def close_kernel(sizes, info_ref, within_ref, readout_ref, cols_ref, states_ref, valve_ref, factor_ref, map_ref, send_ref, keep_ref):
    groups = readout_ref.shape[1] // STATE
    wide = within_ref.shape[1] // groups
    heads = cols_ref.shape[2]
    width = within_ref.shape[1] // heads
    lift_f = spread(jnp.exp(cols_ref[0]), width)
    lift_b = spread(jnp.exp(cols_ref[1]), width)
    blended = []
    for g in range(groups):
        at = slice(g * wide, (g + 1) * wide)
        readout = readout_ref[:, g * STATE : (g + 1) * STATE]
        carried_f = jnp.dot(readout, states_ref[0, :, at], preferred_element_type=jnp.float32)
        carried_b = jnp.dot(readout, states_ref[1, :, at], preferred_element_type=jnp.float32)
        mixed = within_ref[:, at] + carried_f * lift_f[:, at] + carried_b * lift_b[:, at]
        valve = valve_ref[:, at].astype(jnp.float32)
        gated = mixed * (valve / (1.0 + jnp.exp(-valve)))
        square = jnp.mean(gated * gated, axis=1, keepdims=True)
        scaled = gated * lax.rsqrt(square + EPSILON)
        blended.append((scaled * factor_ref[:, at]).astype(jnp.bfloat16))
    rows = jnp.concatenate(blended, axis=1)
    sp_count, count = sizes
    block = map_ref.shape[1] // count
    for p in range(count):
        columns = pl.ds(pl.multiple_of(info_ref[2 * sp_count + p] * block, block), block)
        term = jnp.dot(rows, map_ref[:, columns], preferred_element_type=jnp.float32).astype(jnp.bfloat16)
        target, at = (send_ref, p) if p < count // 2 else (keep_ref, p - count // 2)
        target[:, at * block : (at + 1) * block] = term


def up_kernel(sizes, plan, counts, last, *refs):
    n_pieces, n_arrays = counts
    sp_count, tp_count = sizes
    info_ref, gain_ref = refs[:2]
    pieces = refs[2 : 2 + n_pieces]
    arrays = refs[2 + n_pieces : 2 + n_pieces + n_arrays]
    outs = refs[2 + n_pieces + n_arrays : 4 + n_pieces + n_arrays]
    last_ref, rows_scr, gain_scr = refs[4 + n_pieces + n_arrays :]
    length, full = pieces[0].shape[0], gain_ref.shape[1]
    chunk, block = full // sp_count, full // tp_count
    for p in range(tp_count):
        at = pl.multiple_of(info_ref[2 * sp_count + tp_count + p] * block, block)
        gain_scr[:, p * block : (p + 1) * block] = gain_ref[:, pl.ds(at, block)]

    band = 64

    def norm(r, carry):
        rows = pl.ds(pl.multiple_of(r * band, band), band)
        parts = [piece[rows, :].astype(jnp.float32) for piece in pieces]
        square = sum(jnp.sum(part * part, axis=1, keepdims=True) for part in parts) / full
        factor = lax.rsqrt(square + EPSILON)
        start = 0
        for part in parts:
            for first in range(0, part.shape[1], chunk):
                at = start + first
                rows_scr[at // chunk, rows, :] = (
                    part[:, first : first + chunk] * factor * gain_scr[:, at : at + chunk]
                ).astype(jnp.bfloat16)
            start += part.shape[1]
        return carry

    lax.fori_loop(0, length // band, norm, 0)
    last_ref[...] = rows_scr[info_ref[last] // chunk]
    columns = outs[0].shape[1]
    tile = 256 if columns % 256 == 0 else columns
    for which in range(2):
        for j in range(columns // tile):
            at = slice(j * tile, (j + 1) * tile)
            total = None
            for n, source in enumerate(plan[which]):
                term = jnp.dot(
                    rows_scr[info_ref[source] // chunk],
                    arrays[which * len(plan[0]) + n][:, at],
                    preferred_element_type=jnp.float32,
                )
                total = term if total is None else total + term
            outs[which][:, at] = total


def up_last_kernel(gate_ref, value_ref, rows_ref, gate_map_ref, value_map_ref, gate_out, value_out):
    columns = gate_ref.shape[1]
    tile = 256 if columns % 256 == 0 else columns
    for held, map_ref, out in ((gate_ref, gate_map_ref, gate_out), (value_ref, value_map_ref, value_out)):
        for j in range(columns // tile):
            at = slice(j * tile, (j + 1) * tile)
            term = jnp.dot(rows_ref[...], map_ref[:, at], preferred_element_type=jnp.float32)
            out[:, at] = (held[:, at] + term).astype(jnp.bfloat16)


def down_kernel(sizes, plan, *refs):
    info_ref, hidden_ref = refs[:2]
    arrays, out_ref = refs[2:-1], refs[-1]
    for n, source in enumerate(plan):
        term = down_term(hidden_ref, arrays[2 * n : 2 * n + 2])
        out_ref[info_ref[sizes[0] + source] // term.shape[1]] = term


def down_last_kernel(sizes, plan, blank, band, *refs):
    info_ref, hidden_ref, held_ref = refs[:3]
    arrays, outs = refs[3:-2], refs[-2:]
    count, width = held_ref.shape[0], arrays[0].shape[1]
    columns = slice(band * width, (band + 1) * width)
    both_terms = down_term(hidden_ref, arrays)
    spots = [info_ref[sizes[0] + source] // held_ref.shape[2] for source in plan]
    terms = [both_terms[:, n * width : (n + 1) * width] for n in range(len(plan))]
    spots.append(info_ref[sizes[0] + blank] // held_ref.shape[2])
    terms.append(jnp.zeros_like(terms[0]))
    for p in range(count):
        value = held_ref[p, :, columns]
        for spot, term in zip(spots, terms):
            value = jnp.where(spot == p, term, value)
        side, at = divmod(p * width, outs[0].shape[1])
        outs[side][:, at : at + width] = value


def down_whole_kernel(hidden_ref, map_ref, send_ref, keep_ref):
    half = send_ref.shape[1]
    for out_ref, first in ((send_ref, 0), (keep_ref, half)):
        out_ref[...] = down_term(hidden_ref, [map_ref.at[:, first : first + half]])


def down_term(hidden_ref, parts):
    side_by_side = [part[...] for part in parts]
    whole = side_by_side[0] if len(parts) == 1 else jnp.concatenate(side_by_side, axis=1)
    return jnp.dot(hidden_ref[...], whole, preferred_element_type=jnp.float32).astype(jnp.bfloat16)


def far_kernel(hidden_ref, left_ref, right_ref, out_ref):
    out_ref[...] = down_term(hidden_ref, [left_ref, right_ref])


def conv_rows(padded, kernel, length):
    summed = padded[0:length] * kernel[0]
    for offset in range(1, kernel.shape[0]):
        summed = summed + padded[offset : offset + length] * kernel[offset]
    return summed


def edges(last, first):
    count = lax.axis_size("sp")
    forward = [(i, i + 1) for i in range(count - 1)]
    backward = [(b, a) for a, b in forward]
    low = lax.ppermute(last, "sp", forward)
    high = lax.ppermute(first, "sp", backward)
    return low, high


def call(kernel, outs, *args, scalars=0, scratch=()):
    spaces = [pltpu.SMEM] * scalars + [pltpu.VMEM] * (len(args) - scalars)
    return pl.pallas_call(
        kernel,
        out_shape=[jax.ShapeDtypeStruct(shape, kind) for shape, kind in outs],
        in_specs=[pl.BlockSpec(memory_space=space) for space in spaces],
        scratch_shapes=list(scratch),
        compiler_params=pltpu.CompilerParams(vmem_limit_bytes=LIMIT * 1024 * 1024),
    )(*args)


def solution(mesh):
    cycle = ring_cycle(mesh)
    sp_count = mesh.shape["sp"]
    tp_count = mesh.shape["tp"]
    place = {s: i for i, s in enumerate(cycle)}
    right = [(cycle[i], cycle[(i + 1) % sp_count]) for i in range(sp_count)]
    left = [(b, a) for a, b in right]
    tp = Butterfly(tp_count)
    scatter_place = np.argsort(np.array(tp.scatter_mask))
    gather_place = np.argsort(np.array(tp.gather_mask))

    def table(chunk, own_cols):
        lines = []
        for s in range(sp_count):
            for t in range(tp_count):
                up, down = [], []
                for steps in range(sp_count):
                    block, rest = divmod(cycle[(place[s] - steps) % sp_count] * chunk, own_cols)
                    up.append(gather_place[block ^ t] * own_cols + rest)
                    down.append(scatter_place[block ^ t] * own_cols + rest)
                lines.append(up + down + [t ^ m for m in tp.scatter_mask] + [t ^ m for m in tp.gather_mask])
        return np.array(lines, np.int32)

    def send_on(array, pairs):
        return lax.ppermute(array, "sp", pairs)

    def ring(own, far_ways):
        out = []
        going, coming = own, own
        for step in range(1, (sp_count - 1) // 2 + 1):
            going = send_on(going, right)
            coming = send_on(coming, left)
            out += [(step, going, 0), (-step, coming, 0)]
        if sp_count % 2 == 0:
            far = sp_count // 2
            half = own.shape[0] // 2
            if far_ways == "f":
                out.append((far, send_on(going, right), 0))
            elif far_ways == "b":
                out.append((far, send_on(coming, left), 0))
            else:
                out.append((far, send_on(going[:half], right), 0))
                out.append((far, send_on(coming[half:], left), half))
        return out

    def shards(
        skip_trunk_vector,
        valve_preactivation,
        projected_heads_payload,
        cluster_ingests,
        cluster_observers,
        pre_softplus_increments,
        attenuation_ln_rate,
        additional_attenuation,
        payload_conv_weights,
        ingest_conv_weights,
        observer_conv_weights,
        valved_cluster_factor,
        closing_map_matrix,
        dense_standardize_factor,
        dense_valve_map,
        dense_payload_map,
        valve_series_smoother,
        payload_series_smoother,
        dense_contract_map,
    ):
        length = skip_trunk_vector.shape[0]
        heads = pre_softplus_increments.shape[2]
        channels = projected_heads_payload.shape[1]
        in_cols = cluster_ingests.shape[1]
        own_cols = skip_trunk_vector.shape[1]
        me = lax.axis_index("tp")

        margin = payload_conv_weights.shape[0] // 2
        streams = (projected_heads_payload, cluster_ingests, cluster_observers)
        low, high = edges(
            jnp.concatenate([a[length - margin :] for a in streams], axis=1),
            jnp.concatenate([a[:margin] for a in streams], axis=1),
        )

        full = own_cols * tp_count
        hidden_cols = dense_valve_map.shape[1]
        chunk = dense_valve_map.shape[0]
        up_rings = [[(0, own, 0)] + ring(own, way) for own, way in ((dense_valve_map, "f"), (dense_payload_map, "b"))]
        half_col = chunk // 2
        down_rings = [
            [(0, own, 0)] + ring(own, way)
            for own, way in ((dense_contract_map[:, :half_col], "f"), (dense_contract_map[:, half_col:], "b"))
        ]
        info = jnp.asarray(table(chunk, own_cols))[lax.axis_index("sp") * tp_count + me]

        rows, cols, scale, last = call(
            decay_kernel,
            [
                ((3, heads, length), jnp.float32),
                ((2, length, heads), jnp.float32),
                ((2, length, channels), jnp.float32),
                ((2, 8, channels), jnp.float32),
            ],
            jnp.transpose(pre_softplus_increments, (0, 2, 1)),
            jnp.transpose(additional_attenuation, (0, 2, 1)),
            attenuation_ln_rate.T,
        )

        def mixed(array, low, high, kernel):
            padded = jnp.concatenate([low, array, high], axis=0).astype(jnp.float32)
            return jax.nn.silu(conv_rows(padded, kernel, length)).astype(jnp.bfloat16)

        ends = (channels, channels + in_cols)
        lows, highs = jnp.split(low, ends, axis=1), jnp.split(high, ends, axis=1)
        values = mixed(projected_heads_payload, lows[0], highs[0], payload_conv_weights)
        inputs = mixed(cluster_ingests, lows[1], highs[1], ingest_conv_weights)
        readout = mixed(cluster_observers, lows[2], highs[2], observer_conv_weights)
        wide_state = ((2, STATE + 8, channels), jnp.float32)
        sent = ((STATE + TAIL, channels), jnp.bfloat16)
        window, send_f, send_b = call(
            state_kernel, [wide_state, sent, sent], values, inputs, scale, last
        )
        (within,) = call(
            within_kernel, [((length, channels), jnp.float32)], values, inputs, readout, rows, cols
        )

        before, offset = (), 1
        while offset < sp_count:
            forward = [(i, i + offset) for i in range(sp_count - offset)]
            got_f = lax.ppermute(send_f, "sp", forward)
            got_b = lax.ppermute(send_b, "sp", [(b, a) for a, b in forward])
            final = 2 * offset >= sp_count
            outs = [((2, STATE, channels), jnp.bfloat16)]
            if not final:
                next_sent = ((STATE, channels), jnp.bfloat16) if 4 * offset >= sp_count else sent
                outs = [wide_state, wide_state, next_sent, next_sent]
            result = call(
                functools.partial(link_kernel, offset == 1, final),
                outs,
                got_f,
                got_b,
                *before,
                *(() if final else (window,)),
            )
            if final:
                states = result[0]
            else:
                before, (window, send_f, send_b) = (result[0],), result[1:]
            offset *= 2

        half_full = full // 2
        send, keep = call(
            functools.partial(close_kernel, (sp_count, tp_count)),
            [((length, half_full), jnp.bfloat16)] * 2,
            info,
            within,
            readout,
            cols,
            states,
            valve_preactivation,
            valved_cluster_factor[None, :],
            closing_map_matrix,
            scalars=1,
        )
        projected = tp.reduce_scatter(send, keep)
        middle = (skip_trunk_vector.astype(jnp.float32) + projected).astype(jnp.bfloat16)
        pieces = tp.gather(middle)

        arrays = [array for entries in up_rings for _, array, _ in entries[:-1]]
        plan = [[steps % sp_count for steps, _, _ in entries[:-1]] for entries in up_rings]
        last = up_rings[0][-1][0] % sp_count
        gate_sum, value_sum, last_rows = call(
            functools.partial(up_kernel, (sp_count, tp_count), plan, (len(pieces), len(arrays)), last),
            [((length, hidden_cols), jnp.float32)] * 2 + [((length, chunk), jnp.bfloat16)],
            info,
            dense_standardize_factor[None, :],
            *pieces,
            *arrays,
            scalars=1,
            scratch=[pltpu.VMEM((sp_count, length, chunk), jnp.bfloat16), pltpu.VMEM((1, full), jnp.float32)],
        )
        gate_rows, value_rows = call(
            up_last_kernel,
            [((length, hidden_cols), jnp.bfloat16)] * 2,
            gate_sum,
            value_sum,
            last_rows,
            *(entries[-1][1] for entries in up_rings),
        )
        margin = valve_series_smoother.shape[0] // 2
        low, high = edges(
            jnp.concatenate([gate_rows[length - margin :], value_rows[length - margin :]], axis=1),
            jnp.concatenate([gate_rows[:margin], value_rows[:margin]], axis=1),
        )

        def smooth(array, low, high, kernel):
            return conv_rows(jnp.concatenate([low, array, high], axis=0).astype(jnp.float32), kernel, length)

        gate = smooth(gate_rows, low[:, :hidden_cols], high[:, :hidden_cols], valve_series_smoother)
        value = smooth(value_rows, low[:, hidden_cols:], high[:, hidden_cols:], payload_series_smoother)
        hidden = (jax.nn.silu(gate) * value).astype(jnp.bfloat16)

        halves = [((length, half_full), jnp.bfloat16)] * 2
        if chunk % 256:
            whole = jnp.zeros((hidden_cols, full), jnp.bfloat16)
            for part, entries in enumerate(down_rings):
                for steps, array, _ in entries:
                    corner = (0, info[sp_count + steps % sp_count] + part * half_col)
                    whole = lax.dynamic_update_slice(whole, array, corner)
            send, keep = call(down_whole_kernel, halves, hidden, whole)
            down_sum = tp.reduce_scatter(send, keep)
            return (middle.astype(jnp.float32) + down_sum).astype(jnp.bfloat16)

        far = sp_count // 2
        near_steps = [steps for steps, _, _ in down_rings[0][:-1]]
        held_by = [[array for _, array, _ in entries[:-1]] for entries in down_rings]
        plan = [steps % sp_count for steps in near_steps]
        sizes = (sp_count, tp_count)
        (early,) = call(
            functools.partial(down_kernel, sizes, plan[:-2]),
            [((sp_count, length, chunk), jnp.bfloat16)],
            info,
            hidden,
            *(array for pair in list(zip(*held_by))[:-2] for array in pair),
            scalars=1,
        )
        sums = []
        for band in range(2):
            send, keep = call(
                functools.partial(down_last_kernel, sizes, plan[-2:], far, band),
                [((length, half_full // 2), jnp.bfloat16)] * 2,
                info,
                hidden,
                early,
                *held_by[band][-2:],
                scalars=1,
            )
            sums.append(tp.reduce_scatter(send, keep))
        down_sum = jnp.concatenate(
            [
                band[:, at : at + half_col]
                for at in range(0, own_cols // 2, half_col)
                for band in sums
            ],
            axis=1,
        )
        (part,) = call(
            far_kernel, [((length, chunk), jnp.bfloat16)], hidden, *(entries[-1][1] for entries in down_rings)
        )
        for bit in range(tp.bits):
            pairs = []
            for s in range(sp_count):
                owner = cycle[(place[s] - far) % sp_count] * chunk // own_cols
                for t in range(tp_count):
                    apart = t ^ owner
                    if apart >> bit & 1 and apart % (1 << bit) == 0:
                        pairs.append((s * tp_count + t, s * tp_count + (t ^ (1 << bit))))
            if bit == 0:
                received = tp.swap(part, bit)
            else:
                received = lax.ppermute(part.astype(jnp.bfloat16), ("sp", "tp"), pairs)
            part = part.astype(jnp.float32) + received.astype(jnp.float32)
        at = info[sp_count + far] - (tp_count - 1) * own_cols
        spots = range(0, own_cols, chunk)
        placed = jnp.concatenate([jnp.where(at == spot, part, 0.0) for spot in spots], axis=1)
        return (middle.astype(jnp.float32) + down_sum + placed).astype(jnp.bfloat16)

    return jax.shard_map(
        shards,
        mesh=mesh,
        in_specs=(
            P("sp", "tp"),
            P("sp", "tp"),
            P("sp", "tp"),
            P("sp", "tp"),
            P("sp", "tp"),
            P(None, "sp", "tp"),
            P(None, "tp"),
            P(None, "sp", "tp"),
            P(None, "tp"),
            P(None, "tp"),
            P(None, "tp"),
            P("tp"),
            P("tp", None),
            P(),
            P("sp", "tp"),
            P("sp", "tp"),
            P(None, "tp"),
            P(None, "tp"),
            P("tp", "sp"),
        ),
        out_specs=P("sp", "tp"),
        check_vma=False,
    )
```
